512 devices in a mesh: sp: 16 (over z), dp: 32 (over y, x, core).
Axes of the slice: x: 4, y: 4, z: 16, core: 2. Of those that a mesh axis runs over, the one named last changes fastest.
Arguments:
- cotangent: bfloat16 [32, 2048, 2048], P('dp', 'sp'), may hold values from -6 to 6
- unit_pre: bfloat16 [32, 2048, 2048], P('dp', None, 'sp'), may hold values from -6 to 6
- gate_pre: bfloat16 [32, 2048, 2048], P('dp', None, 'sp'), may hold values from -15 to 15
- out_weight: bfloat16 [2048, 2048], P('dp', 'sp'), may hold values from -0.125 to 0.125
- mix_weight: bfloat16 [8, 128, 128], replicated, may hold values from -0.5 to 0.5
- mix_bias: bfloat16 [8, 128], replicated, may hold values from 0.099609375 to 1.8984375
- norm_gain: bfloat16 [2048], P('sp'), may hold values from 0.099609375 to 1.8984375
- norm_shift: bfloat16 [2048], P('sp'), may hold values from -3 to 3
Outputs:
- unit_grad: bfloat16 [32, 2048, 2048], P('dp', None, 'sp')
- gate_grad: bfloat16 [32, 2048, 2048], P('dp', None, 'sp')
- out_weight_grad: float32 [2048, 2048], P('dp', 'sp')
- mix_weight_grad: float32 [8, 128, 128], replicated
- mix_bias_grad: float32 [8, 128], replicated
- gain_grad: float32 [2048], P('sp')
- shift_grad: float32 [2048], P('sp')
The draws below stay inside these ranges and needn't reach their ends.
All inputs are finite; a program needn't handle non-finite values.
Results may differ from the reference program's by a relative error of at most 0.015.
Values may be sent and summed in bfloat16 or wider, within the bound.
A program may use at most 64 MiB of HBM per device.

```python
import math
import jax
import jax.numpy as jnp
from jax import lax

D = 2048
GW = 2048
GROUPS = 8
BLK = 128
SEQ = 2048
SEQS = 32


def draw_gate_pre(key, part):
    base = jax.random.fold_in(key, 11)
    noise_key, jitter_key = jax.random.split(base, 2)
    position = jnp.arange(GW).astype(jnp.float32) / GW
    jitter = jax.random.uniform(jitter_key, (GW,), jnp.float32, -0.3, 0.3)
    scales = jnp.exp(math.log(0.3) + position * math.log(10.0) + jitter)
    values = jnp.clip(jax.random.normal(noise_key, (SEQS, SEQ, GW), jnp.float32), -3.5, 3.5)
    return (values * scales).astype(jnp.bfloat16)


def block_scale(own_key, shape, shards, least, largest):
    factor_of = 1.0
    for dim, shards_of in shards:
        heights = jax.random.uniform(jax.random.fold_in(jax.random.fold_in(own_key, 6), dim), (shards_of,), jnp.float32, least / len(shards), largest / len(shards))
        factor_of = factor_of * jnp.repeat(jnp.exp(heights), shape[dim] // shards_of).reshape((-1,) + (1,) * (len(shape) - 1 - dim))
    return factor_of


def noise(own_key, extent, width, reach, shards=(), held_as=jnp.bfloat16):
    entries = width * jax.random.normal(own_key, extent, jnp.float32)
    if shards:
        entries = entries * block_scale(own_key, extent, shards, -0.22, 0.18)
    return jnp.clip(entries, -reach, reach).astype(held_as)


def setup_inputs(seed: int = 0) -> dict:
    streams_of = jax.random.split(jax.random.key(seed), 9)
    cotangent = noise(streams_of[0], (SEQS, SEQ, D), 1.0, 6.0, ((0, 32), (1, 16)))
    unit_pre = noise(streams_of[1], (SEQS, SEQ, GW), 1.0, 6.0, ((0, 32), (2, 16)))
    gate_pre = draw_gate_pre(jax.random.fold_in(streams_of[8], 71), 0)
    out_weight = noise(streams_of[3], (D, GW), GW ** -0.5, 0.125, ((0, 32), (1, 16)))
    mix_weight = noise(streams_of[4], (GROUPS, BLK, BLK), BLK ** -0.5, 0.5)
    mix_bias = jnp.clip(1.0 + 0.18 * jax.random.normal(streams_of[5], (GROUPS, BLK), jnp.float32), 0.099609375, 1.8984375).astype(jnp.bfloat16)
    norm_gain = jnp.clip(1.0 + 0.18 * jax.random.normal(streams_of[6], (GW,), jnp.float32), 0.099609375, 1.8984375).astype(jnp.bfloat16)
    norm_shift = noise(streams_of[7], (GW,), 0.5, 3.0, ((0, 16),))
    return {"cotangent": cotangent, "unit_pre": unit_pre, "gate_pre": gate_pre, "out_weight": out_weight, "mix_weight": mix_weight, "mix_bias": mix_bias, "norm_gain": norm_gain, "norm_shift": norm_shift}


epsilon = 1e-05
tanh_coef = math.sqrt(2.0 / math.pi)

def gelu_slope(values):
    inner = tanh_coef * (values + 0.044715 * values * values * values)
    hyper = jnp.tanh(inner)
    return 0.5 * (1.0 + hyper) + 0.5 * values * (1.0 - hyper * hyper) * tanh_coef * (1.0 + 3.0 * 0.044715 * values * values)

def reference(cotangent, unit_pre, gate_pre, out_weight, mix_weight, mix_bias, norm_gain, norm_shift):
    gdim = GW // GROUPS
    blocks = SEQ // BLK
    causal = jnp.arange(BLK)[:, None] >= jnp.arange(BLK)[None, :]
    masked = jnp.where(causal[None], mix_weight.astype(jnp.float32), jnp.float32(0.0))
    bias_full = mix_bias.astype(jnp.float32)
    gain_vec = norm_gain.astype(jnp.float32)
    shift_vec = norm_shift.astype(jnp.float32)

    def one_sequence(totals, inputs):
        dy_seq, unit_seq, gate_seq = inputs
        units = unit_seq.astype(jnp.float32)
        gates = gate_seq.astype(jnp.float32)
        unit_act = jax.nn.gelu(units)
        gate_act = jax.nn.gelu(gates)
        mean_val = lax.optimization_barrier(jnp.mean(gate_act, axis=-1))
        var_val = lax.optimization_barrier(jnp.mean(gate_act * gate_act, axis=-1)) - mean_val * mean_val
        rstd_val = lax.rsqrt(var_val + epsilon)
        centred = (gate_act - mean_val[:, None]) * rstd_val[:, None]
        normed = (centred * gain_vec + shift_vec).astype(jnp.bfloat16)
        normed_blocks = normed.astype(jnp.float32).reshape(blocks, BLK, GROUPS, gdim)
        mixed = jnp.einsum('gts,nsgd->ntgd', masked, normed_blocks) + bias_full.T[None, :, :, None]
        mixed = mixed.reshape(SEQ, GW)
        gated = (unit_act * mixed).astype(jnp.bfloat16)
        head_grad = jnp.dot(dy_seq, out_weight, preferred_element_type=jnp.float32)
        weight_term = lax.dot_general(dy_seq, gated, (((0,), (0,)), ((), ())), preferred_element_type=jnp.float32)
        unit_grad = (head_grad * mixed * gelu_slope(units)).astype(jnp.bfloat16)
        mix_grad = head_grad * unit_act
        mix_round = mix_grad.astype(jnp.bfloat16).astype(jnp.float32).reshape(blocks, BLK, GROUPS, gdim)
        mix_term = jnp.einsum('ntgd,nsgd->gts', mix_round, normed_blocks)
        mix_term = jnp.where(causal[None], mix_term, jnp.float32(0.0))
        bias_term = lax.optimization_barrier(jnp.sum(mix_grad.reshape(blocks, BLK, GROUPS, gdim), axis=(0, 3))).T
        normed_grad = jnp.einsum('gts,ntgd->nsgd', masked, mix_round).reshape(SEQ, GW)
        gain_term = lax.optimization_barrier(jnp.sum(normed_grad * centred, axis=0))
        shift_term = lax.optimization_barrier(jnp.sum(normed_grad, axis=0))
        scaled = normed_grad * gain_vec
        first_m = lax.optimization_barrier(jnp.mean(scaled, axis=-1))
        second_m = lax.optimization_barrier(jnp.mean(scaled * centred, axis=-1))
        gate_grad = (rstd_val[:, None] * (scaled - first_m[:, None] - centred * second_m[:, None]) * gelu_slope(gates)).astype(jnp.bfloat16)
        totals = (totals[0] + weight_term, totals[1] + mix_term, totals[2] + bias_term, totals[3] + gain_term, totals[4] + shift_term)
        return (totals, (unit_grad, gate_grad))
    start_totals = (jnp.zeros((D, GW), jnp.float32), jnp.zeros((GROUPS, BLK, BLK), jnp.float32), jnp.zeros((GROUPS, BLK), jnp.float32), jnp.zeros((GW,), jnp.float32), jnp.zeros((GW,), jnp.float32))
    totals, grads = lax.scan(one_sequence, start_totals, (cotangent, unit_pre, gate_pre))
    token_count = SEQS * SEQ
    norm_scale = 1.0 / math.sqrt(token_count)
    mix_scale = 1.0 / math.sqrt(token_count // BLK * gdim)
    return (grads[0], grads[1], totals[0] * norm_scale, totals[1] * mix_scale, totals[2] * mix_scale, totals[3] * norm_scale, totals[4] * norm_scale)
```

```python
import math

import jax
import jax.numpy as jnp
from jax import lax
from jax.sharding import PartitionSpec as P

GW = 2048
GROUPS = 8
BLK = 128

epsilon = 1e-05
tanh_coef = math.sqrt(2.0 / math.pi)


def sum_over(x, axis):
    devices = lax.axis_size(axis)
    copies = jnp.broadcast_to(x[None], (devices, *x.shape))
    return lax.all_to_all(copies, axis, 0, 0, tiled=True).sum(axis=0)


def gelu_slope(values):
    inner = tanh_coef * (values + 0.044715 * values * values * values)
    hyper = jnp.tanh(inner)
    return 0.5 * (1.0 + hyper) + 0.5 * values * (1.0 - hyper * hyper) * tanh_coef * (
        1.0 + 3.0 * 0.044715 * values * values
    )


def local(cotangent, unit_pre, gate_pre, out_weight, mix_weight, mix_bias, norm_gain, norm_shift):
    seq_len = unit_pre.shape[1]
    channels = unit_pre.shape[2]
    group_dim = GW // GROUPS
    blocks = seq_len // BLK
    sp_size = lax.axis_size("sp")
    sp_at = lax.axis_index("sp")
    group = sp_at * channels // group_dim
    weight_rows = lax.all_gather(out_weight, "sp", axis=1, tiled=True)
    weight_whole = lax.all_gather(weight_rows, "dp", axis=0, tiled=True)
    units = unit_pre[0].astype(jnp.float32)
    gates = gate_pre[0].astype(jnp.float32)
    unit_act = jax.nn.gelu(units)
    gate_act = jax.nn.gelu(gates)
    moments = sum_over(
        jnp.stack([jnp.sum(gate_act, axis=-1), jnp.sum(gate_act * gate_act, axis=-1)]), "sp"
    )
    mean_val = moments[0] / GW
    var_val = moments[1] / GW - mean_val * mean_val
    rstd_val = lax.rsqrt(var_val + epsilon)
    centred = (gate_act - mean_val[:, None]) * rstd_val[:, None]
    gain_vec = norm_gain.astype(jnp.float32)
    normed = (centred * gain_vec + norm_shift.astype(jnp.float32)).astype(jnp.bfloat16)
    causal = jnp.arange(BLK)[:, None] >= jnp.arange(BLK)[None, :]
    local_weight = lax.dynamic_index_in_dim(mix_weight, group, 0, keepdims=False)
    masked = jnp.where(causal, local_weight, jnp.zeros_like(local_weight))
    local_bias = lax.dynamic_index_in_dim(mix_bias, group, 0, keepdims=False).astype(jnp.float32)
    normed_blocks = normed.reshape(blocks, BLK, channels)
    mixed = jnp.einsum("ts,nsd->ntd", masked, normed_blocks, preferred_element_type=jnp.float32)
    mixed = (mixed + local_bias[None, :, None]).reshape(seq_len, channels)
    gated = (unit_act * mixed).astype(jnp.bfloat16)
    gated_rows = lax.all_to_all(gated, "sp", split_axis=0, concat_axis=1, tiled=True)
    head_rows = jnp.dot(cotangent[0], weight_whole, preferred_element_type=jnp.float32)
    head = lax.all_to_all(
        head_rows.astype(jnp.bfloat16), "sp", split_axis=1, concat_axis=0, tiled=True
    ).astype(jnp.float32)
    weight_part = lax.dot_general(
        cotangent[0], gated_rows, (((0,), (0,)), ((), ())), preferred_element_type=jnp.float32
    ).astype(jnp.bfloat16)
    token_count = lax.axis_size("dp") * seq_len
    norm_scale = 1.0 / math.sqrt(token_count)
    mix_scale = 1.0 / math.sqrt(token_count // BLK * group_dim)
    plane_sum = lax.psum_scatter(weight_part, "dp", scatter_dimension=0, tiled=True)
    plane_parts = jnp.moveaxis(plane_sum.reshape(plane_sum.shape[0], sp_size, channels), 1, 0)
    arrived = lax.all_to_all(plane_parts, "sp", split_axis=0, concat_axis=0, tiled=True)
    out_grad = arrived.astype(jnp.float32).sum(axis=0) * norm_scale
    unit_grad = (head * mixed * gelu_slope(units)).astype(jnp.bfloat16)
    mix_grad = head * unit_act
    mix_round = mix_grad.astype(jnp.bfloat16).reshape(blocks, BLK, channels)
    mix_term = jnp.einsum("ntd,nsd->ts", mix_round, normed_blocks, preferred_element_type=jnp.float32)
    mix_term = jnp.where(causal, mix_term, jnp.float32(0.0))
    bias_term = jnp.sum(mix_grad.reshape(blocks, BLK, channels), axis=(0, 2))
    normed_grad = jnp.einsum(
        "ts,ntd->nsd", masked, mix_round, preferred_element_type=jnp.float32
    ).reshape(seq_len, channels)
    gain_term = jnp.sum(normed_grad * centred, axis=0)
    shift_term = jnp.sum(normed_grad, axis=0)
    scaled = normed_grad * gain_vec
    back_sums = sum_over(
        jnp.stack([jnp.sum(scaled, axis=-1), jnp.sum(scaled * centred, axis=-1)]), "sp"
    )
    first_m = back_sums[0] / GW
    second_m = back_sums[1] / GW
    gate_grad = (
        rstd_val[:, None]
        * (scaled - first_m[:, None] - centred * second_m[:, None])
        * gelu_slope(gates)
    ).astype(jnp.bfloat16)
    group_hot = (jnp.arange(GROUPS) == group).astype(jnp.float32)
    own_hot = (jnp.arange(sp_size) == sp_at).astype(jnp.float32)
    packed = jnp.concatenate(
        [
            (group_hot[:, None, None] * mix_term).reshape(GROUPS * BLK, BLK),
            group_hot[:, None] * bias_term,
            own_hot[:, None] * gain_term,
            own_hot[:, None] * shift_term,
        ]
    )
    total = lax.psum(packed, ("sp", "dp"))
    top = GROUPS * BLK
    weight_total = total[:top].reshape(GROUPS, BLK, BLK)
    bias_total = total[top : top + GROUPS]
    tail = total[top + GROUPS :]
    gain_total = lax.dynamic_index_in_dim(tail, sp_at, 0, keepdims=False)
    shift_total = lax.dynamic_index_in_dim(tail, sp_size + sp_at, 0, keepdims=False)
    return (
        unit_grad[None],
        gate_grad[None],
        out_grad,
        weight_total * mix_scale,
        bias_total * mix_scale,
        gain_total * norm_scale,
        shift_total * norm_scale,
    )


def solution(mesh):
    return jax.shard_map(
        local,
        mesh=mesh,
        in_specs=(
            P("dp", "sp", None),
            P("dp", None, "sp"),
            P("dp", None, "sp"),
            P("dp", "sp"),
            P(),
            P(),
            P("sp"),
            P("sp"),
        ),
        out_specs=(P("dp", None, "sp"), P("dp", None, "sp"), P("dp", "sp"), P(), P(), P("sp"), P("sp")),
        check_vma=False,
    )
```

```python
import functools
import math

import jax
import jax.numpy as jnp
from jax import lax
from jax.experimental import pallas as pl
from jax.experimental.pallas import tpu as pltpu
from jax.sharding import PartitionSpec as P

GW = 2048
GROUPS = 8
BLK = 128
MESH = pl.DeviceIdType.MESH

epsilon = 1e-05
tanh_coef = math.sqrt(2.0 / math.pi)


def sent_to_all(x, axis):
    devices = lax.axis_size(axis)
    return lax.all_to_all(jnp.broadcast_to(x[None], (devices, *x.shape)), axis, 0, 0, tiled=True)


def tail_kernel(
    n_sp, n_dp, stats_ref, mix_ref, dw_ref, stats_out, mix_out, dw_out,
    s_buf, s_own, m_buf, w_buf, b_own, b_buf, c_own,
    s1_send, s1_recv, s2_send, s2_recv, m_send, m_recv, w_send, w_recv,
    b_send, b_recv, c_send, c_recv,
):
    sp = lax.axis_index("sp")
    dp = lax.axis_index("dp")

    def sp_at(d):
        return lax.rem(sp + d, n_sp)

    def dp_at(d):
        return lax.rem(dp + d, n_dp)

    def s1(d):
        return pltpu.make_async_remote_copy(
            stats_ref.at[sp_at(d)], s_buf.at[d], s1_send.at[d], s1_recv.at[d],
            device_id={"sp": sp_at(d)}, device_id_type=MESH)

    def s2(d):
        return pltpu.make_async_remote_copy(
            s_own, stats_out.at[sp], s2_send.at[d], s2_recv.at[d],
            device_id={"sp": sp_at(d)}, device_id_type=MESH)

    def m1(d):
        return pltpu.make_async_remote_copy(
            mix_ref.at[dp_at(d)], m_buf.at[d], m_send.at[d], m_recv.at[d],
            device_id={"dp": dp_at(d)}, device_id_type=MESH)

    def w1(d):
        return pltpu.make_async_remote_copy(
            dw_ref.at[dp_at(d)], w_buf.at[d], w_send.at[d], w_recv.at[d],
            device_id={"dp": dp_at(d)}, device_id_type=MESH)

    def b1(d):
        return pltpu.make_async_remote_copy(
            b_own, b_buf.at[sp], b_send.at[d], b_recv.at[d],
            device_id={"sp": sp_at(d)}, device_id_type=MESH)

    def c1(d):
        return pltpu.make_async_remote_copy(
            c_own, mix_out.at[dp], c_send.at[d], c_recv.at[d],
            device_id={"dp": dp_at(d)}, device_id_type=MESH)

    def each(n, f):
        def step(d, carry):
            f(d)
            return carry

        lax.fori_loop(1, n, step, 0)

    barrier = pltpu.get_barrier_semaphore()
    each(n_sp, lambda d: pl.semaphore_signal(
        barrier, inc=1, device_id={"sp": sp_at(d)}, device_id_type=MESH))
    each(n_dp, lambda d: pl.semaphore_signal(
        barrier, inc=1, device_id={"dp": dp_at(d)}, device_id_type=MESH))
    pl.semaphore_wait(barrier, n_sp + n_dp - 2)

    each(n_sp, lambda d: s1(d).start())
    each(n_dp, lambda d: m1(d).start())
    each(n_dp, lambda d: w1(d).start())

    each(n_sp, lambda d: s1(d).wait_recv())
    s_buf[0] = stats_ref[sp]
    total = jnp.sum(s_buf[...], axis=0)
    s_own[...] = total
    stats_out[sp] = total
    each(n_sp, lambda d: s2(d).start())

    each(n_dp, lambda d: m1(d).wait_recv())
    m_buf[0] = mix_ref[dp]
    plane = jnp.sum(m_buf[...], axis=0)
    b_own[...] = plane
    b_buf[sp] = plane
    each(n_sp, lambda d: b1(d).start())

    each(n_dp, lambda d: w1(d).wait_recv())
    w_buf[0] = dw_ref[dp]
    dw_out[...] = jnp.sum(w_buf[...].astype(jnp.float32), axis=0)

    each(n_sp, lambda d: b1(d).wait_recv())
    per = n_sp // GROUPS
    joined = jnp.sum(b_buf[...].reshape(GROUPS, per, 8, BLK), axis=1)
    rows = lax.broadcasted_iota(jnp.int32, (GROUPS, 8, BLK), 1)
    own_plane = jnp.broadcast_to(b_own[...][None], (GROUPS, 8, BLK))
    sent = jnp.where(rows >= 5, own_plane, joined).reshape(GROUPS * 8, BLK).astype(jnp.bfloat16)
    c_own[...] = sent
    mix_out[dp] = sent
    each(n_dp, lambda d: c1(d).start())

    each(n_sp, lambda d: s2(d).wait_recv())
    each(n_dp, lambda d: c1(d).wait_recv())
    each(n_sp, lambda d: s1(d).wait_send())
    each(n_sp, lambda d: s2(d).wait_send())
    each(n_sp, lambda d: b1(d).wait_send())
    each(n_dp, lambda d: m1(d).wait_send())
    each(n_dp, lambda d: w1(d).wait_send())
    each(n_dp, lambda d: c1(d).wait_send())


def finish(stats, mix, dw):
    n_sp, n_dp = lax.axis_size("sp"), lax.axis_size("dp")
    vmem = pl.BlockSpec(memory_space=pltpu.VMEM)
    f32 = jnp.float32
    dma = pltpu.SemaphoreType.DMA
    return pl.pallas_call(
        functools.partial(tail_kernel, n_sp, n_dp),
        out_shape=(
            jax.ShapeDtypeStruct(stats.shape, f32),
            jax.ShapeDtypeStruct((n_dp, GROUPS * 8, BLK), jnp.bfloat16),
            jax.ShapeDtypeStruct(dw.shape[1:], f32),
        ),
        in_specs=[vmem] * 3,
        out_specs=(vmem,) * 3,
        scratch_shapes=[
            pltpu.VMEM(stats.shape, f32),
            pltpu.VMEM(stats.shape[1:], f32),
            pltpu.VMEM(mix.shape, f32),
            pltpu.VMEM(dw.shape, jnp.bfloat16),
            pltpu.VMEM(mix.shape[1:], f32),
            pltpu.VMEM((n_sp, *mix.shape[1:]), f32),
            pltpu.VMEM((GROUPS * 8, BLK), jnp.bfloat16),
            dma((n_sp,)), dma((n_sp,)), dma((n_sp,)), dma((n_sp,)),
            dma((n_dp,)), dma((n_dp,)), dma((n_dp,)), dma((n_dp,)),
            dma((n_sp,)), dma((n_sp,)), dma((n_dp,)), dma((n_dp,)),
        ],
        compiler_params=pltpu.CompilerParams(collective_id=1, has_side_effects=True),
    )(stats, mix, dw)


def gelu_slope(values):
    inner = tanh_coef * (values + 0.044715 * values * values * values)
    hyper = jnp.tanh(inner)
    return 0.5 * (1.0 + hyper) + 0.5 * values * (1.0 - hyper * hyper) * tanh_coef * (
        1.0 + 3.0 * 0.044715 * values * values
    )


def local(cotangent, unit_pre, gate_pre, out_weight, mix_weight, mix_bias, norm_gain, norm_shift):
    seq_len = unit_pre.shape[1]
    channels = unit_pre.shape[2]
    group_dim = GW // GROUPS
    blocks = seq_len // BLK
    n_dp = lax.axis_size("dp")
    group = lax.axis_index("sp") * channels // group_dim
    units = unit_pre[0].astype(jnp.float32)
    gates = gate_pre[0].astype(jnp.float32)
    unit_act = jax.nn.gelu(units)
    gate_act = jax.nn.gelu(gates)
    moments = sent_to_all(
        jnp.stack([jnp.sum(gate_act, axis=-1), jnp.sum(gate_act * gate_act, axis=-1)]), "sp"
    ).sum(axis=0)
    mean_val = moments[0] / GW
    var_val = moments[1] / GW - mean_val * mean_val
    rstd_val = lax.rsqrt(var_val + epsilon)
    centred = (gate_act - mean_val[:, None]) * rstd_val[:, None]
    gain_vec = norm_gain.astype(jnp.float32)
    normed = (centred * gain_vec + norm_shift.astype(jnp.float32)).astype(jnp.bfloat16)
    causal = jnp.arange(BLK)[:, None] >= jnp.arange(BLK)[None, :]
    local_weight = lax.dynamic_index_in_dim(mix_weight, group, 0, keepdims=False)
    masked = jnp.where(causal, local_weight, jnp.zeros_like(local_weight))
    local_bias = lax.dynamic_index_in_dim(mix_bias, group, 0, keepdims=False).astype(jnp.float32)
    normed_blocks = normed.reshape(blocks, BLK, channels)
    mixed = jnp.einsum("ts,nsd->ntd", masked, normed_blocks, preferred_element_type=jnp.float32)
    mixed = (mixed + local_bias[None, :, None]).reshape(seq_len, channels)
    gated = (unit_act * mixed).astype(jnp.bfloat16)
    weight_whole = sent_to_all(out_weight, "dp").reshape(-1, channels)
    dy_rows = lax.all_gather(cotangent, "sp", axis=1, tiled=True)[0]
    head = jnp.dot(dy_rows, weight_whole, preferred_element_type=jnp.float32)
    weight_part = lax.dot_general(
        dy_rows, gated, (((0,), (0,)), ((), ())), preferred_element_type=jnp.float32
    ).astype(jnp.bfloat16)
    token_count = n_dp * seq_len
    norm_scale = 1.0 / math.sqrt(token_count)
    mix_scale = 1.0 / math.sqrt(token_count // BLK * group_dim)
    unit_grad = (head * mixed * gelu_slope(units)).astype(jnp.bfloat16)
    mix_grad = head * unit_act
    mix_round = mix_grad.astype(jnp.bfloat16).reshape(blocks, BLK, channels)
    mix_term = jnp.einsum("ntd,nsd->ts", mix_round, normed_blocks, preferred_element_type=jnp.float32)
    mix_term = jnp.where(causal, mix_term, jnp.float32(0.0))
    bias_term = jnp.sum(mix_grad.reshape(blocks, BLK, channels), axis=(0, 2))
    normed_grad = jnp.einsum(
        "ts,ntd->nsd", masked, mix_round, preferred_element_type=jnp.float32
    ).reshape(seq_len, channels)
    gain_term = jnp.sum(normed_grad * centred, axis=0)
    shift_term = jnp.sum(normed_grad, axis=0)
    scaled = normed_grad * gain_vec
    stats = jnp.stack(
        [
            jnp.sum(scaled, axis=-1).reshape(blocks, BLK),
            jnp.sum(scaled * centred, axis=-1).reshape(blocks, BLK),
        ],
        axis=1,
    )
    small = jnp.stack([bias_term, gain_term, shift_term, jnp.zeros_like(bias_term)])
    first = (jnp.arange(n_dp) == 0)[:, None, None]
    packed = jnp.concatenate(
        [mix_term.reshape(n_dp, BLK // n_dp, BLK), jnp.where(first, small[None], 0.0)], axis=1
    )
    back_sums, mix_all, dw_sum = finish(stats, packed, weight_part.reshape(n_dp, -1, channels))
    first_m = back_sums[:, 0].reshape(seq_len) / GW
    second_m = back_sums[:, 1].reshape(seq_len) / GW
    gate_grad = (
        rstd_val[:, None]
        * (scaled - first_m[:, None] - centred * second_m[:, None])
        * gelu_slope(gates)
    ).astype(jnp.bfloat16)
    mix_all = mix_all.reshape(n_dp, GROUPS, 8, BLK).astype(jnp.float32)
    lines = BLK // n_dp
    weight_total = jnp.swapaxes(mix_all[:, :, :lines], 0, 1).reshape(GROUPS, BLK, BLK)
    return (
        unit_grad[None],
        gate_grad[None],
        dw_sum * norm_scale,
        weight_total * mix_scale,
        mix_all[0, :, 4] * mix_scale,
        mix_all[0, 0, 5] * norm_scale,
        mix_all[0, 0, 6] * norm_scale,
    )


def solution(mesh):
    return jax.shard_map(
        local,
        mesh=mesh,
        in_specs=(
            P("dp", "sp", None),
            P("dp", None, "sp"),
            P("dp", None, "sp"),
            P("dp", "sp"),
            P(),
            P(),
            P("sp"),
            P("sp"),
        ),
        out_specs=(P("dp", None, "sp"), P("dp", None, "sp"), P("dp", "sp"), P(), P(), P("sp"), P("sp")),
        check_vma=False,
    )
```

```python
import functools
import math

import jax
import jax.numpy as jnp
from jax import lax
from jax.experimental import pallas as pl
from jax.experimental.pallas import tpu as pltpu
from jax.sharding import PartitionSpec as P

GROUPS = 8
BLK = 128
MESH = pl.DeviceIdType.MESH
F32 = jnp.float32
BF16 = jnp.bfloat16

epsilon = 1e-05
tanh_coef = math.sqrt(2.0 / math.pi)
SLABS = BLK // 8


def gelu_pair(x):
    hyper = jnp.tanh(tanh_coef * (x + 0.044715 * x * x * x))
    value = 0.5 * x * (1.0 + hyper)
    slope = 0.5 * (1.0 + hyper) + 0.5 * x * (1.0 - hyper * hyper) * tanh_coef * (
        1.0 + 3.0 * 0.044715 * x * x
    )
    return value, slope


def dot(a, b, ca, cb, precision=None):
    return lax.dot_general(
        a, b, (((ca,), (cb,)), ((), ())), preferred_element_type=F32, precision=precision
    )


def row_sums(a, b):
    rows = lax.broadcasted_iota(jnp.int32, (8, 2 * BLK), 0)
    lanes = lax.broadcasted_iota(jnp.int32, (8, 2 * BLK), 1)
    pick = jnp.where(rows == lanes // BLK, 1.0, 0.0).astype(F32)
    both = jnp.concatenate([a, b], axis=1)
    return dot(pick, both, 1, 1, lax.Precision.HIGHEST)[0:2]


def as_columns(pair):
    rows = lax.broadcasted_iota(jnp.int32, (8, 2 * BLK), 0)
    lanes = lax.broadcasted_iota(jnp.int32, (8, 2 * BLK), 1)
    pick = jnp.where(rows == lanes // BLK, 1.0, 0.0).astype(F32)
    padded = jnp.concatenate([pair, jnp.zeros((6, BLK), F32)], axis=0)
    wide = dot(padded, pick, 0, 0, lax.Precision.HIGHEST)
    return wide[:, :BLK], wide[:, BLK:]


def kernel(
    n_sp, n_dp, units_all, norm_scale, mix_scale,
    cot_ref, unit_ref, gate_ref, w_ref, mixw_ref, mixb_ref, gain_ref, shift_ref,
    ugrad_ref, ggrad_ref, dw_out, mix_out, bias_out, gain_out, shift_out,
    gbuf, w_all, gact_s, st_src, st_buf, st_own, st_all,
    bs_src, bs_buf, bs_own, bs_all, masked_s, masked_t, bias_s,
    dwt, scaled_s, cent_s, rs_s, mixacc, bacc, gacc, sacc,
    mix_src, m_buf, w_src, w_buf, b_own, b_buf, c_own, c_buf,
    r_send, r_recv, l_send, l_recv, wa_send, wa_recv,
    f1_send, f1_recv, f2_send, f2_recv, s1_send, s1_recv, s2_send, s2_recv,
    m_send, m_recv, w_send, w_recv, b_send, b_recv, c_send, c_recv,
):
    sp = lax.axis_index("sp")
    dp = lax.axis_index("dp")
    depth = cot_ref.shape[2]
    last = 2 * (n_sp // 2 - 1)

    def sp_at(d):
        return lax.rem(sp + d, n_sp)

    def dp_at(d):
        return lax.rem(dp + d, n_dp)

    right, left = sp_at(1), sp_at(n_sp - 1)

    def each(n, f):
        def step(d, carry):
            f(d)
            return carry

        lax.fori_loop(1, n, step, 0)

    def over_sp(src, dst, send, recv, d):
        return pltpu.make_async_remote_copy(
            src, dst, send.at[d], recv.at[d], device_id={"sp": sp_at(d)}, device_id_type=MESH)

    def over_dp(src, dst, send, recv, d):
        return pltpu.make_async_remote_copy(
            src, dst, send.at[d], recv.at[d], device_id={"dp": dp_at(d)}, device_id_type=MESH)

    def f1(d):
        return over_sp(st_src.at[sp_at(d)], st_buf.at[d], f1_send, f1_recv, d)

    def f2(d):
        return over_sp(st_own, st_all.at[sp], f2_send, f2_recv, d)

    def s1(d):
        return over_sp(bs_src.at[sp_at(d)], bs_buf.at[d], s1_send, s1_recv, d)

    def s2(d):
        return over_sp(bs_own, bs_all.at[sp], s2_send, s2_recv, d)

    def wa(d):
        return over_dp(w_ref, w_all.at[dp], wa_send, wa_recv, d)

    def m1(d):
        return over_dp(mix_src.at[dp_at(d)], m_buf.at[d], m_send, m_recv, d)

    def w1(d):
        return over_dp(w_src.at[dp_at(d)], w_buf.at[d], w_send, w_recv, d)

    def b1(d):
        return over_sp(b_own, b_buf.at[sp], b_send, b_recv, d)

    def c1(d):
        return over_dp(c_own, c_buf.at[dp], c_send, c_recv, d)

    def to_right(src, at, c):
        return pltpu.make_async_remote_copy(
            src, gbuf.at[at], r_send.at[c], r_recv.at[c],
            device_id={"sp": right}, device_id_type=MESH)

    def to_left(src, at, c):
        return pltpu.make_async_remote_copy(
            src, gbuf.at[at], l_send.at[c], l_recv.at[c],
            device_id={"sp": left}, device_id_type=MESH)

    def came_right(c):
        at = 2 * sp_at(n_sp - 1 - c // 2) + lax.rem(c, 2)
        return at, to_right(gbuf.at[at], at, c)

    def came_left(c):
        at = 2 * sp_at(1 + c // 2) + 1 - lax.rem(c, 2)
        return at, to_left(gbuf.at[at], at, c)

    barrier = pltpu.get_barrier_semaphore()
    each(n_sp, lambda d: pl.semaphore_signal(
        barrier, inc=1, device_id={"sp": sp_at(d)}, device_id_type=MESH))
    each(n_dp, lambda d: pl.semaphore_signal(
        barrier, inc=1, device_id={"dp": dp_at(d)}, device_id_type=MESH))

    def gate_sums(p, carry):
        rows = pl.ds(pl.multiple_of(p * BLK, BLK), BLK)
        act, _ = gelu_pair(gate_ref[rows, :].astype(F32))
        gact_s[rows, :] = act
        st_src[p] = row_sums(act, act * act)
        return carry

    lax.fori_loop(0, n_sp, gate_sums, 0)
    pl.semaphore_wait(barrier, n_sp + n_dp - 2)

    each(n_sp, lambda d: f1(d).start())
    for c in range(2):
        to_right(cot_ref.at[c], 2 * sp + c, c).start()
        to_left(cot_ref.at[1 - c], 2 * sp + 1 - c, c).start()
    each(n_dp, lambda d: wa(d).start())

    for c in range(2):
        gbuf[2 * sp + c] = cot_ref[c]
    w_all[dp] = w_ref[...]
    group = sp * GROUPS // n_sp
    t_at = lax.broadcasted_iota(jnp.int32, (BLK, BLK), 0)
    s_at = lax.broadcasted_iota(jnp.int32, (BLK, BLK), 1)
    causal = t_at >= s_at
    masked = jnp.where(causal, mixw_ref[group].astype(F32), 0.0)
    masked_s[...] = masked.astype(BF16)
    masked_t[...] = jnp.transpose(masked).astype(BF16)
    picked = lax.broadcasted_iota(jnp.int32, (GROUPS, BLK), 0) == group
    bias_row = jnp.where(picked, mixb_ref[...].astype(F32), 0.0)
    bias_s[...] = dot(bias_row, jnp.ones((GROUPS, BLK), F32), 0, 0, lax.Precision.HIGHEST)
    for acc in (mixacc, bacc, gacc, sacc, dwt, mix_src):
        acc[...] = jnp.zeros_like(acc)

    each(n_sp, lambda d: f1(d).wait_recv())
    st_buf[0] = st_src[sp]
    moments = jnp.sum(st_buf[...], axis=0) * (1.0 / units_all)
    mean_row = moments[0:1]
    rstd_row = lax.rsqrt(moments[1:2] - mean_row * mean_row + epsilon)
    norm_row = jnp.concatenate([mean_row, rstd_row], axis=0)
    st_own[...] = norm_row
    st_all[sp] = norm_row
    each(n_sp, lambda d: f2(d).start())

    def block(b, carry):
        far = (b + 1) // 2
        d = jnp.where(lax.rem(b, 2) == 1, n_sp - far, far)
        p = sp_at(d)
        rows = pl.ds(pl.multiple_of(p * BLK, BLK), BLK)
        gain = gain_ref[...].astype(F32)
        unit_act, unit_slope = gelu_pair(unit_ref[rows, :].astype(F32))
        _, gate_slope = gelu_pair(gate_ref[rows, :].astype(F32))
        mean, rstd = as_columns(st_all[p])
        centred = (gact_s[rows, :] - mean) * rstd
        normed = (centred * gain + shift_ref[...].astype(F32)).astype(BF16)
        mixed = dot(masked_s[...], normed, 1, 0) + bias_s[...]
        gated = (unit_act * mixed).astype(BF16)
        dy = gbuf[pl.ds(2 * p, 2)].reshape(BLK, depth)
        head = dot(dy, w_all[...].reshape(depth, BLK), 1, 0)
        dwt[...] += dot(gated, dy, 0, 0)
        ugrad_ref[rows, :] = (head * mixed * unit_slope).astype(BF16)
        mix_grad = head * unit_act
        mix_round = mix_grad.astype(BF16)
        mixacc[...] += dot(mix_round, normed, 1, 1)
        bacc[...] += mix_grad
        normed_grad = dot(masked_t[...], mix_round, 1, 0)
        gacc[...] += normed_grad * centred
        sacc[...] += normed_grad
        scaled = normed_grad * gain
        scaled_s[rows, :] = scaled
        cent_s[rows, :] = centred
        rs_s[rows, :] = rstd * gate_slope
        bs_src[p] = row_sums(scaled, scaled * centred)

        @pl.when(b > 0)
        def _():
            s1(d).start()

        return carry

    def step(q, carry):
        @pl.when(q < last)
        def _():
            at, came = came_right(q)
            came.wait_recv()

            @pl.when(q < last - 1)
            def _():
                to_right(gbuf.at[at], at, q + 2).start()

            at_left, came_l = came_left(q)
            came_l.wait_recv()

            @pl.when(q < last - 1)
            def _():
                to_left(gbuf.at[at_left], at_left, q + 2).start()

        @pl.when(q == 2)
        def _():
            each(n_sp, lambda d: f2(d).wait_recv())
            each(n_dp, lambda d: wa(d).wait_recv())

        @pl.when(q == last + 1)
        def _():
            came_right(last)[1].wait_recv()
            came_left(last)[1].wait_recv()

        lo = jnp.maximum(0, jnp.minimum(2 * (q - 2), q))
        hi = jnp.maximum(0, jnp.minimum(2 * (q - 2) + 2, q + 1))
        lax.fori_loop(lo, hi, block, 0)
        return carry

    lax.fori_loop(0, n_sp, step, 0)

    mix_src[0:SLABS] = jnp.where(causal, mixacc[...], 0.0).reshape(SLABS, 8, BLK)
    bias_sum = dot(jnp.ones((8, BLK), F32), bacc[...], 1, 1, lax.Precision.HIGHEST)[0:1]
    mix_src[SLABS] = jnp.concatenate(
        [
            bias_sum,
            jnp.sum(gacc[...], axis=0, keepdims=True),
            jnp.sum(sacc[...], axis=0, keepdims=True),
            jnp.zeros((5, BLK), F32),
        ],
        axis=0,
    )
    each(n_dp, lambda d: m1(d).start())

    piece = depth // n_dp
    per_tile = BLK // piece

    for j in range(depth // BLK):
        tile = jnp.transpose(dwt[:, j * BLK : (j + 1) * BLK]).astype(BF16)
        w_src[j * per_tile : (j + 1) * per_tile] = tile.reshape(per_tile, piece, BLK)
    each(n_dp, lambda d: w1(d).start())

    each(n_sp, lambda d: s1(d).wait_recv())
    bs_buf[0] = bs_src[sp]
    back = jnp.sum(bs_buf[...], axis=0) * (1.0 / units_all)
    bs_own[...] = back
    bs_all[sp] = back
    each(n_sp, lambda d: s2(d).start())

    each(n_dp, lambda d: m1(d).wait_recv())
    m_buf[0] = mix_src[dp]
    plane = jnp.sum(m_buf[...], axis=0)
    b_own[...] = plane
    b_buf[sp] = plane

    @pl.when(dp <= SLABS)
    def _():
        each(n_sp, lambda d: b1(d).start())

    each(n_dp, lambda d: w1(d).wait_recv())
    w_buf[0] = w_src[dp]
    dw_out[...] = jnp.sum(w_buf[...].astype(F32), axis=0) * norm_scale

    @pl.when(dp <= SLABS)
    def _():
        each(n_sp, lambda d: b1(d).wait_recv())
        joined = jnp.sum(b_buf[...].reshape(GROUPS, n_sp // GROUPS, 8, BLK), axis=1)
        at = lax.broadcasted_iota(jnp.int32, (GROUPS, 8, BLK), 1)
        own = jnp.broadcast_to(b_own[...][None], (GROUPS, 8, BLK))
        keep = jnp.logical_and(at >= 1, dp == SLABS)
        sent = jnp.where(keep, own, joined).reshape(GROUPS * 8, BLK).astype(BF16)
        c_own[...] = sent
        c_buf[dp] = sent
        each(n_dp, lambda d: c1(d).start())

    each(n_sp, lambda d: s2(d).wait_recv())

    def gate_block(p, carry):
        rows = pl.ds(pl.multiple_of(p * BLK, BLK), BLK)
        first_m, second_m = as_columns(bs_all[p])
        inner = scaled_s[rows, :] - first_m - cent_s[rows, :] * second_m
        ggrad_ref[rows, :] = (inner * rs_s[rows, :]).astype(BF16)
        return carry

    lax.fori_loop(0, n_sp, gate_block, 0)

    def c_came(d):
        @pl.when(dp_at(n_dp - d) <= SLABS)
        def _():
            c1(d).wait_recv()

    each(n_dp, c_came)
    for i in range(SLABS):
        mix_out[:, 8 * i : 8 * i + 8, :] = (
            c_buf[i].astype(F32).reshape(GROUPS, 8, BLK) * mix_scale
        )
    small = c_buf[SLABS].astype(F32)
    bias_out[...] = jnp.concatenate(
        [small[8 * g : 8 * g + 1] for g in range(GROUPS)], axis=0
    ) * mix_scale
    gain_out[...] = small[1:2] * norm_scale
    shift_out[...] = small[2:3] * norm_scale

    for c in range(2):
        to_right(cot_ref.at[c], 2 * sp + c, c).wait_send()
        to_left(cot_ref.at[1 - c], 2 * sp + 1 - c, c).wait_send()

    def ring_sent(c, carry):
        at = came_right(c - 2)[0]
        to_right(gbuf.at[at], at, c).wait_send()
        at = came_left(c - 2)[0]
        to_left(gbuf.at[at], at, c).wait_send()
        return carry

    lax.fori_loop(2, last + 1, ring_sent, 0)
    each(n_sp, lambda d: f1(d).wait_send())
    each(n_sp, lambda d: f2(d).wait_send())
    each(n_sp, lambda d: s1(d).wait_send())
    each(n_sp, lambda d: s2(d).wait_send())
    each(n_dp, lambda d: wa(d).wait_send())
    each(n_dp, lambda d: m1(d).wait_send())
    each(n_dp, lambda d: w1(d).wait_send())

    @pl.when(dp <= SLABS)
    def _():
        each(n_sp, lambda d: b1(d).wait_send())
        each(n_dp, lambda d: c1(d).wait_send())


def local(cotangent, unit_pre, gate_pre, out_weight, mix_weight, mix_bias, norm_gain, norm_shift):
    n_sp, n_dp = lax.axis_size("sp"), lax.axis_size("dp")
    seq_len, channels = unit_pre.shape[1:]
    depth = cotangent.shape[2]
    units_all = channels * n_sp
    token_count = n_dp * seq_len
    norm_scale = 1.0 / math.sqrt(token_count)
    mix_scale = 1.0 / math.sqrt(token_count // BLK * (units_all // GROUPS))
    piece = depth // n_dp
    vmem = pl.BlockSpec(memory_space=pltpu.VMEM)
    dma = pltpu.SemaphoreType.DMA
    tile = (BLK, BLK)
    chunks = n_sp - 1

    def shape(dims, dtype=F32):
        return jax.ShapeDtypeStruct(dims, dtype)

    outs = pl.pallas_call(
        functools.partial(kernel, n_sp, n_dp, units_all, norm_scale, mix_scale),
        out_shape=(
            shape((seq_len, channels), BF16),
            shape((seq_len, channels), BF16),
            shape((piece, channels)),
            shape((GROUPS, BLK, BLK)),
            shape((GROUPS, BLK)),
            shape((1, channels)),
            shape((1, channels)),
        ),
        in_specs=[vmem] * 8,
        out_specs=(vmem,) * 7,
        scratch_shapes=[
            pltpu.VMEM((2 * n_sp, BLK // 2, depth), BF16),
            pltpu.VMEM((n_dp, piece, channels), BF16),
            pltpu.VMEM((seq_len, channels), F32),
            pltpu.VMEM((n_sp, 2, BLK), F32),
            pltpu.VMEM((n_sp, 2, BLK), F32),
            pltpu.VMEM((2, BLK), F32),
            pltpu.VMEM((n_sp, 2, BLK), F32),
            pltpu.VMEM((n_sp, 2, BLK), F32),
            pltpu.VMEM((n_sp, 2, BLK), F32),
            pltpu.VMEM((2, BLK), F32),
            pltpu.VMEM((n_sp, 2, BLK), F32),
            pltpu.VMEM(tile, BF16),
            pltpu.VMEM(tile, BF16),
            pltpu.VMEM(tile, F32),
            pltpu.VMEM((channels, depth), F32),
            pltpu.VMEM((seq_len, channels), F32),
            pltpu.VMEM((seq_len, channels), F32),
            pltpu.VMEM((seq_len, channels), F32),
            pltpu.VMEM(tile, F32),
            pltpu.VMEM(tile, F32),
            pltpu.VMEM(tile, F32),
            pltpu.VMEM(tile, F32),
            pltpu.VMEM((n_dp, 8, BLK), F32),
            pltpu.VMEM((n_dp, 8, BLK), F32),
            pltpu.VMEM((n_dp, piece, channels), BF16),
            pltpu.VMEM((n_dp, piece, channels), BF16),
            pltpu.VMEM((8, BLK), F32),
            pltpu.VMEM((n_sp, 8, BLK), F32),
            pltpu.VMEM((GROUPS * 8, BLK), BF16),
            pltpu.VMEM((n_dp, GROUPS * 8, BLK), BF16),
            dma((chunks,)), dma((chunks,)), dma((chunks,)), dma((chunks,)),
            dma((n_dp,)), dma((n_dp,)),
            dma((n_sp,)), dma((n_sp,)), dma((n_sp,)), dma((n_sp,)),
            dma((n_sp,)), dma((n_sp,)), dma((n_sp,)), dma((n_sp,)),
            dma((n_dp,)), dma((n_dp,)), dma((n_dp,)), dma((n_dp,)),
            dma((n_sp,)), dma((n_sp,)), dma((n_dp,)), dma((n_dp,)),
        ],
        compiler_params=pltpu.CompilerParams(
            collective_id=1, has_side_effects=True, vmem_limit_bytes=48 << 20
        ),
    )(
        cotangent.reshape(2, BLK // 2, depth),
        unit_pre[0],
        gate_pre[0],
        out_weight,
        mix_weight,
        mix_bias,
        norm_gain[None],
        norm_shift[None],
    )
    unit_grad, gate_grad, out_grad, weight_total, bias_total, gain_total, shift_total = outs
    return (
        unit_grad[None],
        gate_grad[None],
        out_grad,
        weight_total,
        bias_total,
        gain_total[0],
        shift_total[0],
    )


def solution(mesh):
    return jax.shard_map(
        local,
        mesh=mesh,
        in_specs=(
            P("dp", "sp", None),
            P("dp", None, "sp"),
            P("dp", None, "sp"),
            P("dp", "sp"),
            P(),
            P(),
            P("sp"),
            P("sp"),
        ),
        out_specs=(P("dp", None, "sp"), P("dp", None, "sp"), P("dp", "sp"), P(), P(), P("sp"), P("sp")),
        check_vma=False,
    )
```

```python
import functools
import math

import jax
import jax.numpy as jnp
from jax import lax
from jax.experimental import pallas as pl
from jax.experimental.pallas import tpu as pltpu
from jax.sharding import PartitionSpec as P

GROUPS = 8
BLK = 128
MESH = pl.DeviceIdType.MESH
F32 = jnp.float32
BF16 = jnp.bfloat16

epsilon = 1e-05
tanh_coef = math.sqrt(2.0 / math.pi)
ROW = 8
PART = BLK // ROW
NEAR = 5
GRANT = 65_390_000


def gelu_pair(x):
    hyper = jnp.tanh(tanh_coef * (x + 0.044715 * x * x * x))
    value = 0.5 * x * (1.0 + hyper)
    slope = 0.5 * (1.0 + hyper) + 0.5 * x * (1.0 - hyper * hyper) * tanh_coef * (
        1.0 + 3.0 * 0.044715 * x * x
    )
    return value, slope


def dot(a, b, ca, cb, precision=None):
    return lax.dot_general(
        a, b, (((ca,), (cb,)), ((), ())), preferred_element_type=F32, precision=precision
    )


def row_sums(a, b):
    rows = lax.broadcasted_iota(jnp.int32, (8, 2 * BLK), 0)
    lanes = lax.broadcasted_iota(jnp.int32, (8, 2 * BLK), 1)
    pick = jnp.where(rows == lanes // BLK, 1.0, 0.0).astype(F32)
    both = jnp.concatenate([a, b], axis=1)
    return dot(pick, both, 1, 1, lax.Precision.HIGHEST)[0:2]


def as_columns(pair):
    rows = lax.broadcasted_iota(jnp.int32, (8, 2 * BLK), 0)
    lanes = lax.broadcasted_iota(jnp.int32, (8, 2 * BLK), 1)
    pick = jnp.where(rows == lanes // BLK, 1.0, 0.0).astype(F32)
    padded = jnp.concatenate([pair, jnp.zeros((6, BLK), F32)], axis=0)
    wide = dot(padded, pick, 0, 0, lax.Precision.HIGHEST)
    return wide[:, :BLK], wide[:, BLK:]


def kernel(
    n_sp, n_dp, units_all, norm_scale, mix_scale,
    cot_hbm, unit_hbm, gate_hbm, w_hbm, mixw_hbm, mixb_hbm, gain_hbm, shift_hbm,
    ugrad_ref, ggrad_ref, dw_out, mix_out, bias_out, gain_out, shift_out,
    gbuf, w_all, gact_s, st_src, st_buf, st_own, st_all,
    bs_src, bs_buf, bs_own, bs_all, masked_s, masked_t, bias_s,
    dwt, scaled_s, cent_s, rs_s, mixacc, bacc, gacc, sacc,
    mix_src, m_buf, w_src, w_buf, b_own, b_buf, c_own, c_buf,
    late_buf, g_src, g_buf, bias_own, bias_buf,
    unit_ref, gate_ref, mixw_ref, mixb_ref, gain_ref, shift_ref, in_sem,
    r_send, r_recv, l_send, l_recv, wa_send, wa_recv,
    f1_send, f1_recv, f2_send, f2_recv, s1_send, s1_recv, s2_send, s2_recv,
    m_send, m_recv, w_send, w_recv, b_send, b_recv, c_send, c_recv,
    late_send, late_recv, g_send, g_recv, bb_send, bb_recv,
):
    sp = lax.axis_index("sp")
    dp = lax.axis_index("dp")
    depth = cot_hbm.shape[2]
    group = sp * GROUPS // n_sp
    in_row = lax.rem(dp, ROW)
    lates = n_sp - 1 - 2 * NEAR
    last = 2 * (n_sp // 2 - 1)

    def sp_at(d):
        return lax.rem(sp + d, n_sp)

    def dp_at(d):
        return lax.rem(dp + d, n_dp)

    right, left = sp_at(1), sp_at(n_sp - 1)

    def each(n, f):
        def step(d, carry):
            f(d)
            return carry

        lax.fori_loop(1, n, step, 0)

    def over_sp(src, dst, send, recv, d):
        return pltpu.make_async_remote_copy(
            src, dst, send.at[d], recv.at[d], device_id={"sp": sp_at(d)}, device_id_type=MESH)

    def over_dp(src, dst, send, recv, d):
        return pltpu.make_async_remote_copy(
            src, dst, send.at[d], recv.at[d], device_id={"dp": dp_at(d)}, device_id_type=MESH)

    def f1(d):
        return over_sp(st_src.at[sp_at(d)], st_buf.at[d], f1_send, f1_recv, d)

    def f2(d):
        return over_sp(st_own, st_all.at[sp], f2_send, f2_recv, d)

    def s1(d):
        return over_sp(bs_src.at[sp_at(d)], bs_buf.at[d], s1_send, s1_recv, d)

    def s2(d):
        return over_sp(bs_own, bs_all.at[sp], s2_send, s2_recv, d)

    def wa(d):
        return over_dp(w_all.at[dp], w_all.at[dp], wa_send, wa_recv, d)

    def m1(d):
        return over_dp(mix_src.at[lax.rem(dp_at(d), ROW)], m_buf.at[dp], m_send, m_recv, d)

    def g1(d):
        return over_dp(g_src, g_buf.at[dp], g_send, g_recv, d)

    def bb1(d):
        return over_sp(bias_own, bias_buf.at[sp], bb_send, bb_recv, d)

    def late(d, k, p):
        return pltpu.make_async_remote_copy(
            bs_src.at[p], late_buf.at[k, sp], late_send.at[k, d], late_recv.at[k, d],
            device_id={"sp": sp_at(d)}, device_id_type=MESH)

    def w1(d):
        return over_dp(w_src.at[dp_at(d)], w_buf.at[d], w_send, w_recv, d)

    def b1(d):
        return over_sp(b_own, b_buf.at[sp], b_send, b_recv, d)

    def c1(d):
        peer = dp // ROW * ROW + lax.rem(in_row + d, ROW)
        return pltpu.make_async_remote_copy(
            c_own, c_buf.at[in_row], c_send.at[d], c_recv.at[d],
            device_id={"dp": peer}, device_id_type=MESH)

    def to_right(src, at, c):
        return pltpu.make_async_remote_copy(
            src, gbuf.at[at], r_send.at[c], r_recv.at[c],
            device_id={"sp": right}, device_id_type=MESH)

    def to_left(src, at, c):
        return pltpu.make_async_remote_copy(
            src, gbuf.at[at], l_send.at[c], l_recv.at[c],
            device_id={"sp": left}, device_id_type=MESH)

    def came_right(c):
        at = 2 * sp_at(n_sp - 1 - c // 2) + lax.rem(c, 2)
        return at, to_right(gbuf.at[at], at, c)

    def came_left(c):
        at = 2 * sp_at(1 + c // 2) + 1 - lax.rem(c, 2)
        return at, to_left(gbuf.at[at], at, c)

    barrier = pltpu.get_barrier_semaphore()
    each(n_sp, lambda d: pl.semaphore_signal(
        barrier, inc=1, device_id={"sp": sp_at(d)}, device_id_type=MESH))
    each(n_dp, lambda d: pl.semaphore_signal(
        barrier, inc=1, device_id={"dp": dp_at(d)}, device_id_type=MESH))

    loads = [
        pltpu.make_async_copy(src, dst, in_sem.at[i])
        for i, (src, dst) in enumerate(
            [
                (gate_hbm, gate_ref),
                (cot_hbm, gbuf.at[pl.ds(2 * sp, 2)]),
                (w_hbm, w_all.at[dp]),
                (unit_hbm, unit_ref),
                (mixw_hbm.at[group], mixw_ref),
                (mixb_hbm, mixb_ref),
                (gain_hbm, gain_ref),
                (shift_hbm, shift_ref),
            ]
        )
    ]
    for load in loads:
        load.start()
    for acc in (mixacc, bacc, gacc, sacc, dwt):
        acc[...] = jnp.zeros_like(acc)
    loads[0].wait()

    def gate_sums(p, carry):
        rows = pl.ds(pl.multiple_of(p * BLK, BLK), BLK)
        act, _ = gelu_pair(gate_ref[rows, :].astype(F32))
        gact_s[rows, :] = act
        st_src[p] = row_sums(act, act * act)
        return carry

    def own_sends(c):
        at = 2 * sp + c
        back = 2 * sp + 1 - c
        return to_right(gbuf.at[at], at, c), to_left(gbuf.at[back], back, c)

    lax.fori_loop(0, n_sp, gate_sums, 0)
    loads[1].wait()
    pl.semaphore_wait(barrier, n_sp + n_dp - 2)

    each(n_sp, lambda d: f1(d).start())
    for c in range(2):
        for send in own_sends(c):
            send.start()
    loads[2].wait()
    each(n_dp, lambda d: wa(d).start())
    for load in loads[3:]:
        load.wait()

    t_at = lax.broadcasted_iota(jnp.int32, (BLK, BLK), 0)
    s_at = lax.broadcasted_iota(jnp.int32, (BLK, BLK), 1)
    causal = t_at >= s_at
    masked = jnp.where(causal, mixw_ref[...].astype(F32), 0.0)
    masked_s[...] = masked.astype(BF16)
    masked_t[...] = jnp.transpose(masked).astype(BF16)
    picked = lax.broadcasted_iota(jnp.int32, (GROUPS, BLK), 0) == group
    bias_row = jnp.where(picked, mixb_ref[...].astype(F32), 0.0)
    bias_s[...] = dot(bias_row, jnp.ones((GROUPS, BLK), F32), 0, 0, lax.Precision.HIGHEST)

    each(n_sp, lambda d: f1(d).wait_recv())
    st_buf[0] = st_src[sp]
    moments = jnp.sum(st_buf[...], axis=0) * (1.0 / units_all)
    mean_row = moments[0:1]
    rstd_row = lax.rsqrt(moments[1:2] - mean_row * mean_row + epsilon)
    norm_row = jnp.concatenate([mean_row, rstd_row], axis=0)
    st_own[...] = norm_row
    st_all[sp] = norm_row
    each(n_sp, lambda d: f2(d).start())

    def block(b, carry):
        far = (b + 1) // 2
        d = jnp.where(lax.rem(b, 2) == 1, n_sp - far, far)
        p = sp_at(d)
        rows = pl.ds(pl.multiple_of(p * BLK, BLK), BLK)
        gain = gain_ref[...].astype(F32)
        unit_act, unit_slope = gelu_pair(unit_ref[rows, :].astype(F32))
        _, gate_slope = gelu_pair(gate_ref[rows, :].astype(F32))
        mean, rstd = as_columns(st_all[p])
        centred = (gact_s[rows, :] - mean) * rstd
        normed = (centred * gain + shift_ref[...].astype(F32)).astype(BF16)
        mixed = dot(masked_s[...], normed, 1, 0) + bias_s[...]
        gated = (unit_act * mixed).astype(BF16)
        dy = gbuf[pl.ds(2 * p, 2)].reshape(BLK, depth)
        head = dot(dy, w_all[...].reshape(depth, BLK), 1, 0)
        dwt[...] += dot(gated, dy, 0, 0)
        ugrad_ref[rows, :] = (head * mixed * unit_slope).astype(BF16)
        mix_grad = head * unit_act
        mix_round = mix_grad.astype(BF16)
        mixacc[...] += dot(mix_round, normed, 1, 1)
        bacc[...] += mix_grad
        normed_grad = dot(masked_t[...], mix_round, 1, 0)
        gacc[...] += normed_grad * centred
        sacc[...] += normed_grad
        scaled = normed_grad * gain
        scaled_s[rows, :] = scaled
        cent_s[rows, :] = centred
        rs_s[rows, :] = rstd * gate_slope
        sums = row_sums(scaled, scaled * centred)
        bs_src[p] = sums

        @pl.when(jnp.logical_and(b > 0, far <= NEAR))
        def _():
            s1(d).start()

        @pl.when(far > NEAR)
        def _():
            k = d - NEAR - 1
            late_buf[k, sp] = sums
            each(n_sp, lambda e: late(e, k, p).start())

        return carry

    def step(q, carry):
        @pl.when(q < last)
        def _():
            at, came = came_right(q)
            came.wait_recv()

            @pl.when(q < last - 1)
            def _():
                to_right(gbuf.at[at], at, q + 2).start()

            at_left, came_l = came_left(q)
            came_l.wait_recv()

            @pl.when(q < last - 1)
            def _():
                to_left(gbuf.at[at_left], at_left, q + 2).start()

        @pl.when(q == 2)
        def _():
            each(n_sp, lambda d: f2(d).wait_recv())
            each(n_dp, lambda d: wa(d).wait_recv())

        @pl.when(q == last)
        def _():
            def early(d):
                @pl.when(jnp.logical_or(d <= NEAR, d >= n_sp - NEAR))
                def _():
                    s1(d).wait_recv()

            each(n_sp, early)
            own = bs_src[sp]
            for d in range(1, NEAR + 1):
                own = own + bs_buf[d] + bs_buf[n_sp - d]
            bs_own[...] = own
            bs_all[sp] = own
            each(n_sp, lambda d: s2(d).start())

        @pl.when(q == last + 1)
        def _():
            came_right(last)[1].wait_recv()
            came_left(last)[1].wait_recv()

        lo = jnp.maximum(0, jnp.minimum(2 * (q - 2), q))
        hi = jnp.maximum(0, jnp.minimum(2 * (q - 2) + 2, q + 1))
        lax.fori_loop(lo, hi, block, 0)
        return carry

    lax.fori_loop(0, n_sp, step, 0)

    masked_grad = jnp.where(causal, mixacc[...], 0.0).astype(BF16)
    for j in range(ROW):
        mix_src[j] = masked_grad[j * PART : (j + 1) * PART]
    each(n_dp, lambda d: m1(d).start())
    bias_sum = dot(jnp.ones((8, BLK), F32), bacc[...], 1, 1, lax.Precision.HIGHEST)[0:1]
    small = jnp.concatenate(
        [
            bias_sum,
            jnp.sum(gacc[...], axis=0, keepdims=True),
            jnp.sum(sacc[...], axis=0, keepdims=True),
            jnp.zeros((1, BLK), F32),
        ],
        axis=0,
    )
    g_src[...] = small
    g_buf[dp] = small
    m_buf[dp] = mix_src[in_row]
    each(n_dp, lambda d: g1(d).start())

    piece = depth // n_dp
    per_tile = BLK // piece

    for j in range(depth // BLK):
        tile = jnp.transpose(dwt[:, j * BLK : (j + 1) * BLK]).astype(BF16)
        w_src[j * per_tile : (j + 1) * per_tile] = tile.reshape(per_tile, piece, BLK)
    each(n_dp, lambda d: w1(d).start())

    each(n_dp, lambda d: m1(d).wait_recv())
    plane = jnp.sum(m_buf[...].astype(F32), axis=0).astype(BF16)
    b_own[...] = plane
    b_buf[sp] = plane
    each(n_sp, lambda d: b1(d).start())

    each(n_dp, lambda d: g1(d).wait_recv())
    plane_small = jnp.sum(g_buf[...], axis=0)
    gain_out[...] = plane_small[1:2] * norm_scale
    shift_out[...] = plane_small[2:3] * norm_scale
    bias_own[...] = plane_small[0:1]
    bias_buf[sp] = plane_small[0:1]
    each(n_sp, lambda d: bb1(d).start())

    each(n_dp, lambda d: w1(d).wait_recv())
    w_buf[0] = w_src[dp]
    dw_out[...] = jnp.sum(w_buf[...].astype(F32), axis=0) * norm_scale

    each(n_sp, lambda d: s2(d).wait_recv())
    for k in range(lates):
        each(n_sp, lambda d: late(d, k, sp_at(NEAR + 1 + k)).wait_recv())

    def gate_block(p, carry):
        rows = pl.ds(pl.multiple_of(p * BLK, BLK), BLK)
        total = bs_all[p]
        for k in range(lates):
            total = total + late_buf[k, lax.rem(p + n_sp - NEAR - 1 - k, n_sp)]
        first_m, second_m = as_columns(total * (1.0 / units_all))
        inner = scaled_s[rows, :] - first_m - cent_s[rows, :] * second_m
        ggrad_ref[rows, :] = (inner * rs_s[rows, :]).astype(BF16)
        return carry

    def gate_blocks(i, carry):
        for k in range(4):
            gate_block(4 * i + k, carry)
        return carry

    lax.fori_loop(0, n_sp // 4, gate_blocks, 0)

    each(n_sp, lambda d: b1(d).wait_recv())
    joined = jnp.sum(b_buf[...].astype(F32).reshape(GROUPS, n_sp // GROUPS, PART, BLK), axis=1)
    sent = joined.reshape(GROUPS * PART, BLK).astype(BF16)
    c_own[...] = sent
    c_buf[in_row] = sent
    each(ROW, lambda d: c1(d).start())

    each(n_sp, lambda d: bb1(d).wait_recv())
    per = n_sp // GROUPS
    bias_out[...] = jnp.concatenate(
        [sum(bias_buf[per * g + i] for i in range(per)) for g in range(GROUPS)], axis=0
    ) * mix_scale

    each(ROW, lambda d: c1(d).wait_recv())
    for j in range(ROW):
        mix_out[:, PART * j : PART * (j + 1), :] = (
            c_buf[j].astype(F32).reshape(GROUPS, PART, BLK) * mix_scale
        )

    for c in range(2):
        for send in own_sends(c):
            send.wait_send()

    def ring_sent(c, carry):
        at = came_right(c - 2)[0]
        to_right(gbuf.at[at], at, c).wait_send()
        at = came_left(c - 2)[0]
        to_left(gbuf.at[at], at, c).wait_send()
        return carry

    lax.fori_loop(2, last + 1, ring_sent, 0)
    each(n_sp, lambda d: f1(d).wait_send())
    each(n_sp, lambda d: f2(d).wait_send())

    def early_sent(d):
        @pl.when(jnp.logical_or(d <= NEAR, d >= n_sp - NEAR))
        def _():
            s1(d).wait_send()

    each(n_sp, early_sent)
    each(n_sp, lambda d: s2(d).wait_send())
    for k in range(lates):
        each(n_sp, lambda d: late(d, k, sp_at(NEAR + 1 + k)).wait_send())
    each(n_dp, lambda d: wa(d).wait_send())
    each(n_dp, lambda d: m1(d).wait_send())
    each(n_dp, lambda d: g1(d).wait_send())
    each(n_dp, lambda d: w1(d).wait_send())
    each(n_sp, lambda d: b1(d).wait_send())
    each(n_sp, lambda d: bb1(d).wait_send())
    each(ROW, lambda d: c1(d).wait_send())


def put_out(*refs):
    count = len(refs) // 2
    copies = [
        pltpu.make_async_copy(refs[i], refs[count + i], refs[-1].at[i]) for i in range(count)
    ]
    for copy in copies:
        copy.start()
    for copy in copies:
        copy.wait()


def local(cotangent, unit_pre, gate_pre, out_weight, mix_weight, mix_bias, norm_gain, norm_shift):
    n_sp, n_dp = lax.axis_size("sp"), lax.axis_size("dp")
    seq_len, channels = unit_pre.shape[1:]
    depth = cotangent.shape[2]
    units_all = channels * n_sp
    token_count = n_dp * seq_len
    norm_scale = 1.0 / math.sqrt(token_count)
    mix_scale = 1.0 / math.sqrt(token_count // BLK * (units_all // GROUPS))
    piece = depth // n_dp
    vmem = pl.BlockSpec(memory_space=pltpu.VMEM)
    hbm = pl.BlockSpec(memory_space=pltpu.HBM)
    dma = pltpu.SemaphoreType.DMA
    tile = (BLK, BLK)
    chunks = n_sp - 1

    def shape(dims, dtype=F32):
        return jax.ShapeDtypeStruct(dims, dtype)

    out_shapes = (
        shape((seq_len, channels), BF16),
        shape((seq_len, channels), BF16),
        shape((piece, channels)),
        shape((GROUPS, BLK, BLK)),
        shape((GROUPS, BLK)),
        shape((1, channels)),
        shape((1, channels)),
    )
    outs = pl.pallas_call(
        functools.partial(kernel, n_sp, n_dp, units_all, norm_scale, mix_scale),
        out_shape=out_shapes,
        in_specs=[hbm] * 8,
        out_specs=(vmem,) * 7,
        scratch_shapes=[
            pltpu.VMEM((2 * n_sp, BLK // 2, depth), BF16),
            pltpu.VMEM((n_dp, piece, channels), BF16),
            pltpu.VMEM((seq_len, channels), F32),
            pltpu.VMEM((n_sp, 2, BLK), F32),
            pltpu.VMEM((n_sp, 2, BLK), F32),
            pltpu.VMEM((2, BLK), F32),
            pltpu.VMEM((n_sp, 2, BLK), F32),
            pltpu.VMEM((n_sp, 2, BLK), F32),
            pltpu.VMEM((n_sp, 2, BLK), F32),
            pltpu.VMEM((2, BLK), F32),
            pltpu.VMEM((n_sp, 2, BLK), F32),
            pltpu.VMEM(tile, BF16),
            pltpu.VMEM(tile, BF16),
            pltpu.VMEM(tile, F32),
            pltpu.VMEM((channels, depth), F32),
            pltpu.VMEM((seq_len, channels), F32),
            pltpu.VMEM((seq_len, channels), F32),
            pltpu.VMEM((seq_len, channels), F32),
            pltpu.VMEM(tile, F32),
            pltpu.VMEM(tile, F32),
            pltpu.VMEM(tile, F32),
            pltpu.VMEM(tile, F32),
            pltpu.VMEM((ROW, PART, BLK), BF16),
            pltpu.VMEM((n_dp, PART, BLK), BF16),
            pltpu.VMEM((n_dp, piece, channels), BF16),
            pltpu.VMEM((n_dp, piece, channels), BF16),
            pltpu.VMEM((PART, BLK), BF16),
            pltpu.VMEM((n_sp, PART, BLK), BF16),
            pltpu.VMEM((GROUPS * PART, BLK), BF16),
            pltpu.VMEM((ROW, GROUPS * PART, BLK), BF16),
            pltpu.VMEM((n_sp - 1 - 2 * NEAR, n_sp, 2, BLK), F32),
            pltpu.VMEM((4, BLK), F32),
            pltpu.VMEM((n_dp, 4, BLK), F32),
            pltpu.VMEM((1, BLK), F32),
            pltpu.VMEM((n_sp, 1, BLK), F32),
            pltpu.VMEM((seq_len, channels), BF16),
            pltpu.VMEM((seq_len, channels), BF16),
            pltpu.VMEM(tile, BF16),
            pltpu.VMEM((GROUPS, BLK), BF16),
            pltpu.VMEM((1, channels), BF16),
            pltpu.VMEM((1, channels), BF16),
            dma((8,)),
            dma((chunks,)), dma((chunks,)), dma((chunks,)), dma((chunks,)),
            dma((n_dp,)), dma((n_dp,)),
            dma((n_sp,)), dma((n_sp,)), dma((n_sp,)), dma((n_sp,)),
            dma((n_sp,)), dma((n_sp,)), dma((n_sp,)), dma((n_sp,)),
            dma((n_dp,)), dma((n_dp,)), dma((n_dp,)), dma((n_dp,)),
            dma((n_sp,)), dma((n_sp,)), dma((ROW,)), dma((ROW,)),
            dma((n_sp - 1 - 2 * NEAR, n_sp)), dma((n_sp - 1 - 2 * NEAR, n_sp)),
            dma((n_dp,)), dma((n_dp,)), dma((n_sp,)), dma((n_sp,)),
        ],
        compiler_params=pltpu.CompilerParams(
            collective_id=1, has_side_effects=True, vmem_limit_bytes=GRANT
        ),
    )(
        cotangent.reshape(2, BLK // 2, depth),
        unit_pre[0],
        gate_pre[0],
        out_weight,
        mix_weight,
        mix_bias,
        norm_gain[None],
        norm_shift[None],
    )
    outs = pl.pallas_call(
        put_out,
        out_shape=out_shapes,
        in_specs=[vmem] * 7,
        out_specs=(hbm,) * 7,
        scratch_shapes=[dma((7,))],
        compiler_params=pltpu.CompilerParams(vmem_limit_bytes=GRANT),
    )(*outs)
    unit_grad, gate_grad, out_grad, weight_total, bias_total, gain_total, shift_total = outs
    return (
        unit_grad[None],
        gate_grad[None],
        out_grad,
        weight_total,
        bias_total,
        gain_total[0],
        shift_total[0],
    )


def solution(mesh):
    return jax.shard_map(
        local,
        mesh=mesh,
        in_specs=(
            P("dp", "sp", None),
            P("dp", None, "sp"),
            P("dp", None, "sp"),
            P("dp", "sp"),
            P(),
            P(),
            P("sp"),
            P("sp"),
        ),
        out_specs=(P("dp", None, "sp"), P("dp", None, "sp"), P("dp", "sp"), P(), P(), P("sp"), P("sp")),
        check_vma=False,
    )
```

```python
import functools
import math

import jax
import jax.numpy as jnp
from jax import lax
from jax.experimental import pallas as pl
from jax.experimental.pallas import tpu as pltpu
from jax.sharding import PartitionSpec as P

GROUPS = 8
BLK = 128
MESH = pl.DeviceIdType.MESH
F32 = jnp.float32
BF16 = jnp.bfloat16

epsilon = 1e-05
tanh_coef = math.sqrt(2.0 / math.pi)
ROW = 8
SIDE = 4
FIRST = 4
PART = BLK // ROW
GRANT = 65_390_000


def gelu_pair(x):
    hyper = jnp.tanh(tanh_coef * (x + 0.044715 * x * x * x))
    value = 0.5 * x * (1.0 + hyper)
    slope = 0.5 * (1.0 + hyper) + 0.5 * x * (1.0 - hyper * hyper) * tanh_coef * (
        1.0 + 3.0 * 0.044715 * x * x
    )
    return value, slope


def dot(a, b, ca, cb, precision=None):
    return lax.dot_general(
        a, b, (((ca,), (cb,)), ((), ())), preferred_element_type=F32, precision=precision
    )


def row_sums(a, b):
    rows = lax.broadcasted_iota(jnp.int32, (8, 2 * BLK), 0)
    lanes = lax.broadcasted_iota(jnp.int32, (8, 2 * BLK), 1)
    pick = jnp.where(rows == lanes // BLK, 1.0, 0.0).astype(F32)
    both = jnp.concatenate([a, b], axis=1)
    return dot(pick, both, 1, 1, lax.Precision.HIGHEST)[0:2]


def as_columns(pair):
    rows = lax.broadcasted_iota(jnp.int32, (8, 2 * BLK), 0)
    lanes = lax.broadcasted_iota(jnp.int32, (8, 2 * BLK), 1)
    pick = jnp.where(rows == lanes // BLK, 1.0, 0.0).astype(F32)
    padded = jnp.concatenate([pair, jnp.zeros((6, BLK), F32)], axis=0)
    wide = dot(padded, pick, 0, 0, lax.Precision.HIGHEST)
    return wide[:, :BLK], wide[:, BLK:]


def kernel(
    n_sp, n_dp, units_all, norm_scale, mix_scale,
    cot_hbm, unit_hbm, gate_hbm, w_hbm, mixw_hbm, mixb_hbm, gain_hbm, shift_hbm,
    ugrad_ref, ggrad_ref, dw_out, mix_out, bias_out, gain_out, shift_out,
    gbuf, w_all, gact_s, st_src, st_buf, st_own, st_all,
    bs_src, bs_buf, bs_own, bs_all, masked_s, masked_t, bias_s,
    dwt, scaled_s, cent_s, rs_s, mixacc, bacc, gacc, sacc,
    mix_src, m_buf, w_src, w_buf, b_own, b_buf, c_own, c_buf,
    g_src, g_buf, bias_own, bias_buf,
    unit_ref, gate_ref, mixw_ref, mixb_ref, gain_ref, shift_ref, in_sem,
    r_send, r_recv, l_send, l_recv, wa_send, wa_recv,
    f1_send, f1_recv, f2_send, f2_recv, s1_send, s1_recv, s2_send, s2_recv,
    m_send, m_recv, w_send, w_recv, b_send, b_recv, c_send, c_recv,
    g_send, g_recv, bb_send, bb_recv, met,
):
    sp = lax.axis_index("sp")
    dp = lax.axis_index("dp")
    depth = cot_hbm.shape[2]
    group = sp * GROUPS // n_sp
    in_row = lax.rem(dp, ROW)
    last = 2 * (n_sp // 2 - 1)

    def sp_at(d):
        return lax.rem(sp + d, n_sp)

    def dp_at(d):
        return lax.rem(dp + d, n_dp)

    right, left = sp_at(1), sp_at(n_sp - 1)

    def each(n, f):
        def step(d, carry):
            f(d)
            return carry

        lax.fori_loop(1, n, step, 0)

    def over_sp(src, dst, send, recv, d):
        return pltpu.make_async_remote_copy(
            src, dst, send.at[d], recv.at[d], device_id={"sp": sp_at(d)}, device_id_type=MESH)

    def over_dp(src, dst, send, recv, d):
        return pltpu.make_async_remote_copy(
            src, dst, send.at[d], recv.at[d], device_id={"dp": dp_at(d)}, device_id_type=MESH)

    def f1(d):
        return over_sp(st_src.at[sp_at(d)], st_buf.at[d], f1_send, f1_recv, d)

    def f2(d):
        return over_sp(st_own, st_all.at[sp], f2_send, f2_recv, d)

    def s1(d):
        return over_sp(bs_src.at[sp_at(d)], bs_buf.at[d], s1_send, s1_recv, d)

    def s2(d):
        return over_sp(bs_own, bs_all.at[sp], s2_send, s2_recv, d)

    def wa(d):
        return over_dp(w_all.at[dp], w_all.at[dp], wa_send, wa_recv, d)

    def m1(d):
        return over_dp(mix_src.at[lax.rem(dp_at(d), ROW)], m_buf.at[dp], m_send, m_recv, d)

    def g1(d):
        return over_dp(g_src, g_buf.at[dp], g_send, g_recv, d)

    def bb1(d):
        return over_sp(bias_own, bias_buf.at[sp], bb_send, bb_recv, d)

    def w1(d):
        return over_dp(w_src.at[dp_at(d)], w_buf.at[d], w_send, w_recv, d)

    def b1(d):
        return over_sp(b_own, b_buf.at[sp], b_send, b_recv, d)

    def c1(d):
        peer = dp // ROW * ROW + lax.rem(in_row + d, ROW)
        return pltpu.make_async_remote_copy(
            c_own, c_buf.at[in_row], c_send.at[d], c_recv.at[d],
            device_id={"dp": peer}, device_id_type=MESH)

    def to_right(src, at, c):
        return pltpu.make_async_remote_copy(
            src, gbuf.at[at], r_send.at[c], r_recv.at[c],
            device_id={"sp": right}, device_id_type=MESH)

    def to_left(src, at, c):
        return pltpu.make_async_remote_copy(
            src, gbuf.at[at], l_send.at[c], l_recv.at[c],
            device_id={"sp": left}, device_id_type=MESH)

    def came_right(c):
        at = 2 * sp_at(n_sp - 1 - c // 2) + lax.rem(c, 2)
        return at, to_right(gbuf.at[at], at, c)

    def came_left(c):
        at = 2 * sp_at(1 + c // 2) + 1 - lax.rem(c, 2)
        return at, to_left(gbuf.at[at], at, c)

    core, x_at, y_at = lax.rem(dp, 2), lax.rem(dp // 2, SIDE), dp // (2 * SIDE)

    def in_plane(dy, dx, dc):
        line = lax.rem(y_at + dy, SIDE) * SIDE + lax.rem(x_at + dx, SIDE)
        return {"dp": line * 2 + lax.rem(core + dc, 2)}

    def greet(sem, peers):
        for peer in peers:
            pl.semaphore_signal(sem, inc=1, device_id=peer, device_id_type=MESH)

    around = [in_plane(0, 0, 1), in_plane(0, 1, 0), in_plane(0, SIDE - 1, 0)]
    around += [in_plane(1, 0, 0), in_plane(SIDE - 1, 0, 0), {"sp": right}, {"sp": left}]
    across = [in_plane(0, 0, 1), in_plane(0, SIDE // 2, 0), in_plane(SIDE // 2, 0, 0)]
    rounds = [
        around,
        across + [{"sp": sp_at(2)}, {"sp": sp_at(n_sp - 2)}],
        across + [{"sp": sp_at(4)}, {"sp": sp_at(n_sp - 4)}],
    ]
    barrier = pltpu.get_barrier_semaphore()
    greet(barrier, around)

    loads = [
        pltpu.make_async_copy(src, dst, in_sem.at[i])
        for i, (src, dst) in enumerate(
            [
                (gate_hbm, gate_ref),
                (cot_hbm, gbuf.at[pl.ds(2 * sp, 2)]),
                (w_hbm, w_all.at[dp]),
                (unit_hbm, unit_ref),
                (mixw_hbm.at[group], mixw_ref),
                (mixb_hbm, mixb_ref),
                (gain_hbm, gain_ref),
                (shift_hbm, shift_ref),
            ]
        )
    ]
    for load in loads:
        load.start()
    for acc in (mixacc, bacc, gacc, sacc, dwt):
        acc[...] = jnp.zeros_like(acc)

    def gate_sums(p, carry):
        rows = pl.ds(pl.multiple_of(p * BLK, BLK), BLK)
        act, _ = gelu_pair(gate_ref[rows, :].astype(F32))
        gact_s[rows, :] = act
        st_src[p] = row_sums(act, act * act)
        return carry

    def own_sends(c):
        at = 2 * sp + c
        back = 2 * sp + 1 - c
        return to_right(gbuf.at[at], at, c), to_left(gbuf.at[back], back, c)

    loads[1].wait()
    pl.semaphore_wait(barrier, len(around))
    for c in range(2):
        for send in own_sends(c):
            send.start()
    loads[0].wait()
    bounds = [0, n_sp // 2, n_sp, n_sp]
    for r, peers in enumerate(rounds):
        greet(met.at[r], peers)
        lax.fori_loop(bounds[r], bounds[r + 1], gate_sums, 0)
        pl.semaphore_wait(met.at[r], len(peers))

    each(n_sp, lambda d: f1(d).start())
    loads[2].wait()
    each(n_dp, lambda d: wa(d).start())
    for load in loads[3:]:
        load.wait()

    t_at = lax.broadcasted_iota(jnp.int32, (BLK, BLK), 0)
    s_at = lax.broadcasted_iota(jnp.int32, (BLK, BLK), 1)
    causal = t_at >= s_at
    masked = jnp.where(causal, mixw_ref[...].astype(F32), 0.0)
    masked_s[...] = masked.astype(BF16)
    masked_t[...] = jnp.transpose(masked).astype(BF16)
    picked = lax.broadcasted_iota(jnp.int32, (GROUPS, BLK), 0) == group
    bias_row = jnp.where(picked, mixb_ref[...].astype(F32), 0.0)
    bias_s[...] = dot(bias_row, jnp.ones((GROUPS, BLK), F32), 0, 0, lax.Precision.HIGHEST)

    each(n_sp, lambda d: f1(d).wait_recv())
    st_buf[0] = st_src[sp]
    moments = jnp.sum(st_buf[...], axis=0) * (1.0 / units_all)
    mean_row = moments[0:1]
    rstd_row = lax.rsqrt(moments[1:2] - mean_row * mean_row + epsilon)
    norm_row = jnp.concatenate([mean_row, rstd_row], axis=0)
    st_own[...] = norm_row
    st_all[sp] = norm_row
    each(n_sp, lambda d: f2(d).start())

    def block(b, carry):
        far = (b + 1) // 2
        d = jnp.where(lax.rem(b, 2) == 1, n_sp - far, far)
        p = sp_at(d)
        rows = pl.ds(pl.multiple_of(p * BLK, BLK), BLK)
        gain = gain_ref[...].astype(F32)
        unit_act, unit_slope = gelu_pair(unit_ref[rows, :].astype(F32))
        _, gate_slope = gelu_pair(gate_ref[rows, :].astype(F32))
        mean, rstd = as_columns(st_all[p])
        centred = (gact_s[rows, :] - mean) * rstd
        normed = (centred * gain + shift_ref[...].astype(F32)).astype(BF16)
        mixed = dot(masked_s[...], normed, 1, 0) + bias_s[...]
        gated = (unit_act * mixed).astype(BF16)
        dy = gbuf[pl.ds(2 * p, 2)].reshape(BLK, depth)
        head = dot(dy, w_all[...].reshape(depth, BLK), 1, 0)
        dwt[...] += dot(gated, dy, 0, 0)
        ugrad_ref[rows, :] = (head * mixed * unit_slope).astype(BF16)
        mix_grad = head * unit_act
        mix_round = mix_grad.astype(BF16)
        mixacc[...] += dot(mix_round, normed, 1, 1)
        bacc[...] += mix_grad
        normed_grad = dot(masked_t[...], mix_round, 1, 0)
        gacc[...] += normed_grad * centred
        sacc[...] += normed_grad
        scaled = normed_grad * gain
        scaled_s[rows, :] = scaled
        cent_s[rows, :] = centred
        rs_s[rows, :] = rstd * gate_slope
        bs_src[p] = row_sums(scaled, scaled * centred)

        @pl.when(b > 0)
        def _():
            s1(d).start()

        return carry

    def step(q, carry):
        @pl.when(q < last)
        def _():
            at, came = came_right(q)
            came.wait_recv()

            @pl.when(q < last - 1)
            def _():
                to_right(gbuf.at[at], at, q + 2).start()

            at_left, came_l = came_left(q)
            came_l.wait_recv()

            @pl.when(q < last - 1)
            def _():
                to_left(gbuf.at[at_left], at_left, q + 2).start()

        @pl.when(q == FIRST)
        def _():
            each(n_sp, lambda d: f2(d).wait_recv())
            each(n_dp, lambda d: wa(d).wait_recv())

        @pl.when(q == last + 1)
        def _():
            came_right(last)[1].wait_recv()
            came_left(last)[1].wait_recv()

        lo = jnp.maximum(0, jnp.minimum(2 * (q - FIRST), q))
        hi = jnp.maximum(0, jnp.minimum(2 * (q - FIRST) + 2, q + 1))
        lax.fori_loop(lo, hi, block, 0)
        return carry

    lax.fori_loop(0, n_sp, step, 0)

    masked_grad = jnp.where(causal, mixacc[...], 0.0).astype(BF16)
    for j in range(ROW):
        mix_src[j] = masked_grad[j * PART : (j + 1) * PART]
    each(n_dp, lambda d: m1(d).start())
    bias_sum = dot(jnp.ones((8, BLK), F32), bacc[...], 1, 1, lax.Precision.HIGHEST)[0:1]
    small = jnp.concatenate(
        [
            bias_sum,
            jnp.sum(gacc[...], axis=0, keepdims=True),
            jnp.sum(sacc[...], axis=0, keepdims=True),
            jnp.zeros((1, BLK), F32),
        ],
        axis=0,
    )
    g_src[...] = small
    g_buf[dp] = small
    m_buf[dp] = mix_src[in_row]
    each(n_dp, lambda d: g1(d).start())

    piece = depth // n_dp
    per_tile = BLK // piece

    for j in range(depth // BLK):
        tile = jnp.transpose(dwt[:, j * BLK : (j + 1) * BLK]).astype(BF16)
        w_src[j * per_tile : (j + 1) * per_tile] = tile.reshape(per_tile, piece, BLK)
    each(n_dp, lambda d: w1(d).start())

    each(n_dp, lambda d: m1(d).wait_recv())
    plane = jnp.sum(m_buf[...].astype(F32), axis=0).astype(BF16)
    b_own[...] = plane
    b_buf[sp] = plane
    each(n_sp, lambda d: b1(d).start())

    each(n_sp, lambda d: s1(d).wait_recv())
    bs_buf[0] = bs_src[sp]
    back = jnp.sum(bs_buf[...], axis=0) * (1.0 / units_all)
    bs_own[...] = back
    bs_all[sp] = back
    each(n_sp, lambda d: s2(d).start())

    each(n_dp, lambda d: g1(d).wait_recv())
    plane_small = jnp.sum(g_buf[...], axis=0)
    gain_out[...] = plane_small[1:2] * norm_scale
    shift_out[...] = plane_small[2:3] * norm_scale
    bias_own[...] = plane_small[0:1]
    bias_buf[sp] = plane_small[0:1]
    each(n_sp, lambda d: bb1(d).start())

    each(n_dp, lambda d: w1(d).wait_recv())
    w_buf[0] = w_src[dp]
    dw_out[...] = jnp.sum(w_buf[...].astype(F32), axis=0) * norm_scale

    each(n_sp, lambda d: b1(d).wait_recv())
    joined = jnp.sum(b_buf[...].astype(F32).reshape(GROUPS, n_sp // GROUPS, PART, BLK), axis=1)
    sent = joined.reshape(GROUPS * PART, BLK).astype(BF16)
    c_own[...] = sent
    c_buf[in_row] = sent
    each(ROW, lambda d: c1(d).start())

    each(n_sp, lambda d: s2(d).wait_recv())

    def gate_block(p):
        rows = pl.ds(pl.multiple_of(p * BLK, BLK), BLK)
        first_m, second_m = as_columns(bs_all[p])
        inner = scaled_s[rows, :] - first_m - cent_s[rows, :] * second_m
        ggrad_ref[rows, :] = (inner * rs_s[rows, :]).astype(BF16)

    def gate_blocks(i, carry):
        for k in range(4):
            gate_block(4 * i + k)
        return carry

    lax.fori_loop(0, n_sp // 4, gate_blocks, 0)

    each(n_sp, lambda d: bb1(d).wait_recv())
    per = n_sp // GROUPS
    bias_out[...] = jnp.concatenate(
        [sum(bias_buf[per * g + i] for i in range(per)) for g in range(GROUPS)], axis=0
    ) * mix_scale

    each(ROW, lambda d: c1(d).wait_recv())
    for j in range(ROW):
        mix_out[:, PART * j : PART * (j + 1), :] = (
            c_buf[j].astype(F32).reshape(GROUPS, PART, BLK) * mix_scale
        )

    for c in range(2):
        for send in own_sends(c):
            send.wait_send()

    def ring_sent(c, carry):
        at = came_right(c - 2)[0]
        to_right(gbuf.at[at], at, c).wait_send()
        at = came_left(c - 2)[0]
        to_left(gbuf.at[at], at, c).wait_send()
        return carry

    lax.fori_loop(2, last + 1, ring_sent, 0)
    each(n_sp, lambda d: f1(d).wait_send())
    each(n_sp, lambda d: f2(d).wait_send())

    each(n_sp, lambda d: s1(d).wait_send())
    each(n_sp, lambda d: s2(d).wait_send())
    each(n_dp, lambda d: wa(d).wait_send())
    each(n_dp, lambda d: m1(d).wait_send())
    each(n_dp, lambda d: g1(d).wait_send())
    each(n_dp, lambda d: w1(d).wait_send())
    each(n_sp, lambda d: b1(d).wait_send())
    each(n_sp, lambda d: bb1(d).wait_send())
    each(ROW, lambda d: c1(d).wait_send())


def put_out(*refs):
    count = len(refs) // 2
    copies = [
        pltpu.make_async_copy(refs[i], refs[count + i], refs[-1].at[i]) for i in range(count)
    ]
    for copy in copies:
        copy.start()
    for copy in copies:
        copy.wait()


def local(cotangent, unit_pre, gate_pre, out_weight, mix_weight, mix_bias, norm_gain, norm_shift):
    n_sp, n_dp = lax.axis_size("sp"), lax.axis_size("dp")
    seq_len, channels = unit_pre.shape[1:]
    depth = cotangent.shape[2]
    units_all = channels * n_sp
    token_count = n_dp * seq_len
    norm_scale = 1.0 / math.sqrt(token_count)
    mix_scale = 1.0 / math.sqrt(token_count // BLK * (units_all // GROUPS))
    piece = depth // n_dp
    vmem = pl.BlockSpec(memory_space=pltpu.VMEM)
    hbm = pl.BlockSpec(memory_space=pltpu.HBM)
    dma = pltpu.SemaphoreType.DMA
    tile = (BLK, BLK)
    chunks = n_sp - 1

    def shape(dims, dtype=F32):
        return jax.ShapeDtypeStruct(dims, dtype)

    out_shapes = (
        shape((seq_len, channels), BF16),
        shape((seq_len, channels), BF16),
        shape((piece, channels)),
        shape((GROUPS, BLK, BLK)),
        shape((GROUPS, BLK)),
        shape((1, channels)),
        shape((1, channels)),
    )
    outs = pl.pallas_call(
        functools.partial(kernel, n_sp, n_dp, units_all, norm_scale, mix_scale),
        out_shape=out_shapes,
        in_specs=[hbm] * 8,
        out_specs=(vmem,) * 7,
        scratch_shapes=[
            pltpu.VMEM((2 * n_sp, BLK // 2, depth), BF16),
            pltpu.VMEM((n_dp, piece, channels), BF16),
            pltpu.VMEM((seq_len, channels), F32),
            pltpu.VMEM((n_sp, 2, BLK), F32),
            pltpu.VMEM((n_sp, 2, BLK), F32),
            pltpu.VMEM((2, BLK), F32),
            pltpu.VMEM((n_sp, 2, BLK), F32),
            pltpu.VMEM((n_sp, 2, BLK), F32),
            pltpu.VMEM((n_sp, 2, BLK), F32),
            pltpu.VMEM((2, BLK), F32),
            pltpu.VMEM((n_sp, 2, BLK), F32),
            pltpu.VMEM(tile, BF16),
            pltpu.VMEM(tile, BF16),
            pltpu.VMEM(tile, F32),
            pltpu.VMEM((channels, depth), F32),
            pltpu.VMEM((seq_len, channels), F32),
            pltpu.VMEM((seq_len, channels), F32),
            pltpu.VMEM((seq_len, channels), F32),
            pltpu.VMEM(tile, F32),
            pltpu.VMEM(tile, F32),
            pltpu.VMEM(tile, F32),
            pltpu.VMEM(tile, F32),
            pltpu.VMEM((ROW, PART, BLK), BF16),
            pltpu.VMEM((n_dp, PART, BLK), BF16),
            pltpu.VMEM((n_dp, piece, channels), BF16),
            pltpu.VMEM((n_dp, piece, channels), BF16),
            pltpu.VMEM((PART, BLK), BF16),
            pltpu.VMEM((n_sp, PART, BLK), BF16),
            pltpu.VMEM((GROUPS * PART, BLK), BF16),
            pltpu.VMEM((ROW, GROUPS * PART, BLK), BF16),
            pltpu.VMEM((4, BLK), F32),
            pltpu.VMEM((n_dp, 4, BLK), F32),
            pltpu.VMEM((1, BLK), F32),
            pltpu.VMEM((n_sp, 1, BLK), F32),
            pltpu.VMEM((seq_len, channels), BF16),
            pltpu.VMEM((seq_len, channels), BF16),
            pltpu.VMEM(tile, BF16),
            pltpu.VMEM((GROUPS, BLK), BF16),
            pltpu.VMEM((1, channels), BF16),
            pltpu.VMEM((1, channels), BF16),
            dma((8,)),
            dma((chunks,)), dma((chunks,)), dma((chunks,)), dma((chunks,)),
            dma((n_dp,)), dma((n_dp,)),
            dma((n_sp,)), dma((n_sp,)), dma((n_sp,)), dma((n_sp,)),
            dma((n_sp,)), dma((n_sp,)), dma((n_sp,)), dma((n_sp,)),
            dma((n_dp,)), dma((n_dp,)), dma((n_dp,)), dma((n_dp,)),
            dma((n_sp,)), dma((n_sp,)), dma((ROW,)), dma((ROW,)),
            dma((n_dp,)), dma((n_dp,)), dma((n_sp,)), dma((n_sp,)),
            pltpu.SemaphoreType.REGULAR((3,)),
        ],
        compiler_params=pltpu.CompilerParams(
            collective_id=1, has_side_effects=True, vmem_limit_bytes=GRANT
        ),
    )(
        cotangent.reshape(2, BLK // 2, depth),
        unit_pre[0],
        gate_pre[0],
        out_weight,
        mix_weight,
        mix_bias,
        norm_gain[None],
        norm_shift[None],
    )
    outs = pl.pallas_call(
        put_out,
        out_shape=out_shapes,
        in_specs=[vmem] * 7,
        out_specs=(hbm,) * 7,
        scratch_shapes=[dma((7,))],
        compiler_params=pltpu.CompilerParams(vmem_limit_bytes=GRANT),
    )(*outs)
    unit_grad, gate_grad, out_grad, weight_total, bias_total, gain_total, shift_total = outs
    return (
        unit_grad[None],
        gate_grad[None],
        out_grad,
        weight_total,
        bias_total,
        gain_total[0],
        shift_total[0],
    )


def solution(mesh):
    return jax.shard_map(
        local,
        mesh=mesh,
        in_specs=(
            P("dp", "sp", None),
            P("dp", None, "sp"),
            P("dp", None, "sp"),
            P("dp", "sp"),
            P(),
            P(),
            P("sp"),
            P("sp"),
        ),
        out_specs=(P("dp", None, "sp"), P("dp", None, "sp"), P("dp", "sp"), P(), P(), P("sp"), P("sp")),
        check_vma=False,
    )
```

```python
import functools
import math

import jax
import jax.numpy as jnp
from jax import lax
from jax.experimental import pallas as pl
from jax.experimental.pallas import tpu as pltpu
from jax.sharding import PartitionSpec as P

GROUPS = 8
BLK = 128
MESH = pl.DeviceIdType.MESH
F32 = jnp.float32
BF16 = jnp.bfloat16

epsilon = 1e-05
tanh_coef = math.sqrt(2.0 / math.pi)
ROW = 8
SIDE = 4
SUMS = 2
FIRST = 6
PART = BLK // ROW
GRANT = 65_390_000


def gelu_pair(x):
    hyper = jnp.tanh(tanh_coef * (x + 0.044715 * x * x * x))
    value = 0.5 * x * (1.0 + hyper)
    slope = 0.5 * (1.0 + hyper) + 0.5 * x * (1.0 - hyper * hyper) * tanh_coef * (
        1.0 + 3.0 * 0.044715 * x * x
    )
    return value, slope


def dot(a, b, ca, cb, precision=None):
    return lax.dot_general(
        a, b, (((ca,), (cb,)), ((), ())), preferred_element_type=F32, precision=precision
    )


def row_sums(a, b):
    rows = lax.broadcasted_iota(jnp.int32, (8, 2 * BLK), 0)
    lanes = lax.broadcasted_iota(jnp.int32, (8, 2 * BLK), 1)
    pick = jnp.where(rows == lanes // BLK, 1.0, 0.0).astype(F32)
    both = jnp.concatenate([a, b], axis=1)
    return dot(pick, both, 1, 1, lax.Precision.HIGHEST)[0:2]


def as_columns(pair):
    rows = lax.broadcasted_iota(jnp.int32, (8, 2 * BLK), 0)
    lanes = lax.broadcasted_iota(jnp.int32, (8, 2 * BLK), 1)
    pick = jnp.where(rows == lanes // BLK, 1.0, 0.0).astype(F32)
    padded = jnp.concatenate([pair, jnp.zeros((6, BLK), F32)], axis=0)
    wide = dot(padded, pick, 0, 0, lax.Precision.HIGHEST)
    return wide[:, :BLK], wide[:, BLK:]


def kernel(
    n_sp, n_dp, units_all, norm_scale, mix_scale,
    cot_hbm, unit_hbm, gate_hbm, w_hbm, mixw_hbm, mixb_hbm, gain_hbm, shift_hbm,
    ugrad_ref, ggrad_ref, dw_out, mix_out, bias_out, gain_out, shift_out,
    gbuf, w_all, gact_s, st_src, st_buf, st_own, st_all,
    bs_src, bs_buf, bs_own, bs_all, masked_s, masked_t, bias_s,
    dwt, scaled_s, cent_s, rs_s, mixacc, bacc, gacc, sacc,
    mix_src, m_buf, w_src, w_buf, b_own, b_buf, c_own, c_buf,
    g_src, g_buf, bias_own, bias_buf,
    unit_ref, gate_ref, mixw_ref, mixb_ref, gain_ref, shift_ref, in_sem,
    r_send, r_recv, l_send, l_recv, wa_send, wa_recv,
    f1_send, f1_recv, f2_send, f2_recv, s1_send, s1_recv, s2_send, s2_recv,
    m_send, m_recv, w_send, w_recv, b_send, b_recv, c_send, c_recv,
    g_send, g_recv, bb_send, bb_recv, met,
):
    sp = lax.axis_index("sp")
    dp = lax.axis_index("dp")
    depth = cot_hbm.shape[2]
    group = sp * GROUPS // n_sp
    in_row = lax.rem(dp, ROW)
    last = 2 * (n_sp // 2 - 1)

    def sp_at(d):
        return lax.rem(sp + d, n_sp)

    def dp_at(d):
        return lax.rem(dp + d, n_dp)

    right, left = sp_at(1), sp_at(n_sp - 1)

    def each(n, f):
        def step(d, carry):
            f(d)
            return carry

        lax.fori_loop(1, n, step, 0)

    def over_sp(src, dst, send, recv, d):
        return pltpu.make_async_remote_copy(
            src, dst, send.at[d], recv.at[d], device_id={"sp": sp_at(d)}, device_id_type=MESH)

    def over_dp(src, dst, send, recv, d):
        return pltpu.make_async_remote_copy(
            src, dst, send.at[d], recv.at[d], device_id={"dp": dp_at(d)}, device_id_type=MESH)

    def f1(d):
        return over_sp(st_src.at[sp_at(d)], st_buf.at[d], f1_send, f1_recv, d)

    def f2(d):
        return over_sp(st_own, st_all.at[sp], f2_send, f2_recv, d)

    def s1(d):
        return over_sp(bs_src.at[sp_at(d)], bs_buf.at[d], s1_send, s1_recv, d)

    def s2(d):
        return over_sp(bs_own, bs_all.at[sp], s2_send, s2_recv, d)

    def wa(d):
        return over_dp(w_all.at[dp], w_all.at[dp], wa_send, wa_recv, d)

    def m1(d):
        return over_dp(mix_src.at[lax.rem(dp_at(d), ROW)], m_buf.at[dp], m_send, m_recv, d)

    def g1(d):
        return over_dp(g_src, g_buf.at[dp], g_send, g_recv, d)

    def bb1(d):
        return over_sp(bias_own, bias_buf.at[sp], bb_send, bb_recv, d)

    def w1(d):
        return over_dp(w_src.at[dp_at(d)], w_buf.at[d], w_send, w_recv, d)

    def b1(d):
        return over_sp(b_own, b_buf.at[sp], b_send, b_recv, d)

    def c1(d):
        peer = dp // ROW * ROW + lax.rem(in_row + d, ROW)
        return pltpu.make_async_remote_copy(
            c_own, c_buf.at[in_row], c_send.at[d], c_recv.at[d],
            device_id={"dp": peer}, device_id_type=MESH)

    def to_right(src, at, c):
        return pltpu.make_async_remote_copy(
            src, gbuf.at[at], r_send.at[c], r_recv.at[c],
            device_id={"sp": right}, device_id_type=MESH)

    def to_left(src, at, c):
        return pltpu.make_async_remote_copy(
            src, gbuf.at[at], l_send.at[c], l_recv.at[c],
            device_id={"sp": left}, device_id_type=MESH)

    def came_right(c):
        at = 2 * sp_at(n_sp - 1 - c // 2) + lax.rem(c, 2)
        return at, to_right(gbuf.at[at], at, c)

    def came_left(c):
        at = 2 * sp_at(1 + c // 2) + 1 - lax.rem(c, 2)
        return at, to_left(gbuf.at[at], at, c)

    core, x_at, y_at = lax.rem(dp, 2), lax.rem(dp // 2, SIDE), dp // (2 * SIDE)

    def in_plane(dy, dx, dc):
        line = lax.rem(y_at + dy, SIDE) * SIDE + lax.rem(x_at + dx, SIDE)
        return {"dp": line * 2 + lax.rem(core + dc, 2)}

    def greet(sem, peers):
        for peer in peers:
            pl.semaphore_signal(sem, inc=1, device_id=peer, device_id_type=MESH)

    around = [in_plane(0, 0, 1), in_plane(0, 1, 0), in_plane(0, SIDE - 1, 0)]
    around += [in_plane(1, 0, 0), in_plane(SIDE - 1, 0, 0), {"sp": right}, {"sp": left}]
    across = [in_plane(0, 0, 1), in_plane(0, SIDE // 2, 0), in_plane(SIDE // 2, 0, 0)]
    rounds = [
        around,
        across + [{"sp": sp_at(2)}, {"sp": sp_at(n_sp - 2)}],
        across + [{"sp": sp_at(4)}, {"sp": sp_at(n_sp - 4)}],
    ]
    barrier = pltpu.get_barrier_semaphore()
    greet(barrier, around)

    loads = [
        pltpu.make_async_copy(src, dst, in_sem.at[i])
        for i, (src, dst) in enumerate(
            [
                (gate_hbm, gate_ref),
                (cot_hbm, gbuf.at[pl.ds(2 * sp, 2)]),
                (w_hbm, w_all.at[dp]),
                (unit_hbm, unit_ref),
                (mixw_hbm.at[group], mixw_ref),
                (mixb_hbm, mixb_ref),
                (gain_hbm, gain_ref),
                (shift_hbm, shift_ref),
            ]
        )
    ]
    for load in loads:
        load.start()
    for acc in (mixacc, bacc, gacc, sacc, dwt):
        acc[...] = jnp.zeros_like(acc)

    def gate_sums(p, carry):
        rows = pl.ds(pl.multiple_of(p * BLK, BLK), BLK)
        act, _ = gelu_pair(gate_ref[rows, :].astype(F32))
        gact_s[rows, :] = act
        st_src[p] = row_sums(act, act * act)
        return carry

    def own_sends(c):
        at = 2 * sp + c
        back = 2 * sp + 1 - c
        return to_right(gbuf.at[at], at, c), to_left(gbuf.at[back], back, c)

    loads[1].wait()
    pl.semaphore_wait(barrier, len(around))
    for c in range(2):
        for send in own_sends(c):
            send.start()
    loads[0].wait()
    bounds = [0, n_sp // 2, n_sp, n_sp]
    for r, peers in enumerate(rounds):
        greet(met.at[r], peers)
        lax.fori_loop(bounds[r], bounds[r + 1], gate_sums, 0)
        pl.semaphore_wait(met.at[r], len(peers))

    each(n_sp, lambda d: f1(d).start())
    loads[2].wait()
    each(n_dp, lambda d: wa(d).start())
    for load in loads[3:]:
        load.wait()

    t_at = lax.broadcasted_iota(jnp.int32, (BLK, BLK), 0)
    s_at = lax.broadcasted_iota(jnp.int32, (BLK, BLK), 1)
    causal = t_at >= s_at
    masked = jnp.where(causal, mixw_ref[...].astype(F32), 0.0)
    masked_s[...] = masked.astype(BF16)
    masked_t[...] = jnp.transpose(masked).astype(BF16)
    picked = lax.broadcasted_iota(jnp.int32, (GROUPS, BLK), 0) == group
    bias_row = jnp.where(picked, mixb_ref[...].astype(F32), 0.0)
    bias_s[...] = dot(bias_row, jnp.ones((GROUPS, BLK), F32), 0, 0, lax.Precision.HIGHEST)

    def block(b, carry):
        far = (b + 1) // 2
        d = jnp.where(lax.rem(b, 2) == 1, n_sp - far, far)
        p = sp_at(d)
        rows = pl.ds(pl.multiple_of(p * BLK, BLK), BLK)
        gain = gain_ref[...].astype(F32)
        unit_act, unit_slope = gelu_pair(unit_ref[rows, :].astype(F32))
        _, gate_slope = gelu_pair(gate_ref[rows, :].astype(F32))
        mean, rstd = as_columns(st_all[p])
        centred = (gact_s[rows, :] - mean) * rstd
        normed = (centred * gain + shift_ref[...].astype(F32)).astype(BF16)
        mixed = dot(masked_s[...], normed, 1, 0) + bias_s[...]
        gated = (unit_act * mixed).astype(BF16)
        dy = gbuf[pl.ds(2 * p, 2)].reshape(BLK, depth)
        head = dot(dy, w_all[...].reshape(depth, BLK), 1, 0)
        dwt[...] += dot(gated, dy, 0, 0)
        ugrad_ref[rows, :] = (head * mixed * unit_slope).astype(BF16)
        mix_grad = head * unit_act
        mix_round = mix_grad.astype(BF16)
        mixacc[...] += dot(mix_round, normed, 1, 1)
        bacc[...] += mix_grad
        normed_grad = dot(masked_t[...], mix_round, 1, 0)
        gacc[...] += normed_grad * centred
        sacc[...] += normed_grad
        scaled = normed_grad * gain
        scaled_s[rows, :] = scaled
        cent_s[rows, :] = centred
        rs_s[rows, :] = rstd * gate_slope
        bs_src[p] = row_sums(scaled, scaled * centred)

        @pl.when(b > 0)
        def _():
            s1(d).start()

        return carry

    def step(q, carry):
        @pl.when(q < last)
        def _():
            at, came = came_right(q)
            came.wait_recv()

            @pl.when(q < last - 1)
            def _():
                to_right(gbuf.at[at], at, q + 2).start()

            at_left, came_l = came_left(q)
            came_l.wait_recv()

            @pl.when(q < last - 1)
            def _():
                to_left(gbuf.at[at_left], at_left, q + 2).start()

        @pl.when(q == SUMS)
        def _():
            each(n_sp, lambda d: f1(d).wait_recv())
            st_buf[0] = st_src[sp]
            moments = jnp.sum(st_buf[...], axis=0) * (1.0 / units_all)
            mean_row = moments[0:1]
            rstd_row = lax.rsqrt(moments[1:2] - mean_row * mean_row + epsilon)
            norm_row = jnp.concatenate([mean_row, rstd_row], axis=0)
            st_own[...] = norm_row
            st_all[sp] = norm_row
            each(n_sp, lambda d: f2(d).start())

        @pl.when(q == FIRST)
        def _():
            each(n_sp, lambda d: f2(d).wait_recv())
            each(n_dp, lambda d: wa(d).wait_recv())

        @pl.when(q == last + 1)
        def _():
            came_right(last)[1].wait_recv()
            came_left(last)[1].wait_recv()

        lo = jnp.maximum(0, jnp.minimum(2 * (q - FIRST), q))
        hi = jnp.maximum(0, jnp.minimum(2 * (q - FIRST) + 2, q + 1))
        lax.fori_loop(lo, hi, block, 0)
        return carry

    lax.fori_loop(0, n_sp, step, 0)

    masked_grad = jnp.where(causal, mixacc[...], 0.0).astype(BF16)
    for j in range(ROW):
        mix_src[j] = masked_grad[j * PART : (j + 1) * PART]
    each(n_dp, lambda d: m1(d).start())
    bias_sum = dot(jnp.ones((8, BLK), F32), bacc[...], 1, 1, lax.Precision.HIGHEST)[0:1]
    small = jnp.concatenate(
        [
            bias_sum,
            jnp.sum(gacc[...], axis=0, keepdims=True),
            jnp.sum(sacc[...], axis=0, keepdims=True),
            jnp.zeros((1, BLK), F32),
        ],
        axis=0,
    )
    g_src[...] = small
    g_buf[dp] = small
    m_buf[dp] = mix_src[in_row]
    each(n_dp, lambda d: g1(d).start())

    piece = depth // n_dp
    per_tile = BLK // piece

    for j in range(depth // BLK):
        tile = jnp.transpose(dwt[:, j * BLK : (j + 1) * BLK]).astype(BF16)
        w_src[j * per_tile : (j + 1) * per_tile] = tile.reshape(per_tile, piece, BLK)
    each(n_dp, lambda d: w1(d).start())

    each(n_dp, lambda d: m1(d).wait_recv())
    plane = jnp.sum(m_buf[...].astype(F32), axis=0).astype(BF16)
    b_own[...] = plane
    b_buf[sp] = plane
    each(n_sp, lambda d: b1(d).start())

    each(n_sp, lambda d: s1(d).wait_recv())
    bs_buf[0] = bs_src[sp]
    back = jnp.sum(bs_buf[...], axis=0) * (1.0 / units_all)
    bs_own[...] = back
    bs_all[sp] = back
    each(n_sp, lambda d: s2(d).start())

    each(n_dp, lambda d: g1(d).wait_recv())
    plane_small = jnp.sum(g_buf[...], axis=0)
    gain_out[...] = plane_small[1:2] * norm_scale
    shift_out[...] = plane_small[2:3] * norm_scale
    bias_own[...] = plane_small[0:1]
    bias_buf[sp] = plane_small[0:1]
    each(n_sp, lambda d: bb1(d).start())

    each(n_dp, lambda d: w1(d).wait_recv())
    w_buf[0] = w_src[dp]
    dw_out[...] = jnp.sum(w_buf[...].astype(F32), axis=0) * norm_scale

    each(n_sp, lambda d: b1(d).wait_recv())
    joined = jnp.sum(b_buf[...].astype(F32).reshape(GROUPS, n_sp // GROUPS, PART, BLK), axis=1)
    sent = joined.reshape(GROUPS * PART, BLK).astype(BF16)
    c_own[...] = sent
    c_buf[in_row] = sent
    each(ROW, lambda d: c1(d).start())

    each(n_sp, lambda d: s2(d).wait_recv())

    def gate_block(p):
        rows = pl.ds(pl.multiple_of(p * BLK, BLK), BLK)
        first_m, second_m = as_columns(bs_all[p])
        inner = scaled_s[rows, :] - first_m - cent_s[rows, :] * second_m
        ggrad_ref[rows, :] = (inner * rs_s[rows, :]).astype(BF16)

    def gate_blocks(i, carry):
        for k in range(4):
            gate_block(4 * i + k)
        return carry

    lax.fori_loop(0, n_sp // 4, gate_blocks, 0)

    each(n_sp, lambda d: bb1(d).wait_recv())
    per = n_sp // GROUPS
    bias_out[...] = jnp.concatenate(
        [sum(bias_buf[per * g + i] for i in range(per)) for g in range(GROUPS)], axis=0
    ) * mix_scale

    each(ROW, lambda d: c1(d).wait_recv())
    for j in range(ROW):
        mix_out[:, PART * j : PART * (j + 1), :] = (
            c_buf[j].astype(F32).reshape(GROUPS, PART, BLK) * mix_scale
        )

    for c in range(2):
        for send in own_sends(c):
            send.wait_send()

    def ring_sent(c, carry):
        at = came_right(c - 2)[0]
        to_right(gbuf.at[at], at, c).wait_send()
        at = came_left(c - 2)[0]
        to_left(gbuf.at[at], at, c).wait_send()
        return carry

    lax.fori_loop(2, last + 1, ring_sent, 0)
    each(n_sp, lambda d: f1(d).wait_send())
    each(n_sp, lambda d: f2(d).wait_send())

    each(n_sp, lambda d: s1(d).wait_send())
    each(n_sp, lambda d: s2(d).wait_send())
    each(n_dp, lambda d: wa(d).wait_send())
    each(n_dp, lambda d: m1(d).wait_send())
    each(n_dp, lambda d: g1(d).wait_send())
    each(n_dp, lambda d: w1(d).wait_send())
    each(n_sp, lambda d: b1(d).wait_send())
    each(n_sp, lambda d: bb1(d).wait_send())
    each(ROW, lambda d: c1(d).wait_send())


def put_out(*refs):
    count = len(refs) // 2
    copies = [
        pltpu.make_async_copy(refs[i], refs[count + i], refs[-1].at[i]) for i in range(count)
    ]
    for copy in copies:
        copy.start()
    for copy in copies:
        copy.wait()


def local(cotangent, unit_pre, gate_pre, out_weight, mix_weight, mix_bias, norm_gain, norm_shift):
    n_sp, n_dp = lax.axis_size("sp"), lax.axis_size("dp")
    seq_len, channels = unit_pre.shape[1:]
    depth = cotangent.shape[2]
    units_all = channels * n_sp
    token_count = n_dp * seq_len
    norm_scale = 1.0 / math.sqrt(token_count)
    mix_scale = 1.0 / math.sqrt(token_count // BLK * (units_all // GROUPS))
    piece = depth // n_dp
    vmem = pl.BlockSpec(memory_space=pltpu.VMEM)
    hbm = pl.BlockSpec(memory_space=pltpu.HBM)
    dma = pltpu.SemaphoreType.DMA
    tile = (BLK, BLK)
    chunks = n_sp - 1

    def shape(dims, dtype=F32):
        return jax.ShapeDtypeStruct(dims, dtype)

    out_shapes = (
        shape((seq_len, channels), BF16),
        shape((seq_len, channels), BF16),
        shape((piece, channels)),
        shape((GROUPS, BLK, BLK)),
        shape((GROUPS, BLK)),
        shape((1, channels)),
        shape((1, channels)),
    )
    outs = pl.pallas_call(
        functools.partial(kernel, n_sp, n_dp, units_all, norm_scale, mix_scale),
        out_shape=out_shapes,
        in_specs=[hbm] * 8,
        out_specs=(vmem,) * 7,
        scratch_shapes=[
            pltpu.VMEM((2 * n_sp, BLK // 2, depth), BF16),
            pltpu.VMEM((n_dp, piece, channels), BF16),
            pltpu.VMEM((seq_len, channels), F32),
            pltpu.VMEM((n_sp, 2, BLK), F32),
            pltpu.VMEM((n_sp, 2, BLK), F32),
            pltpu.VMEM((2, BLK), F32),
            pltpu.VMEM((n_sp, 2, BLK), F32),
            pltpu.VMEM((n_sp, 2, BLK), F32),
            pltpu.VMEM((n_sp, 2, BLK), F32),
            pltpu.VMEM((2, BLK), F32),
            pltpu.VMEM((n_sp, 2, BLK), F32),
            pltpu.VMEM(tile, BF16),
            pltpu.VMEM(tile, BF16),
            pltpu.VMEM(tile, F32),
            pltpu.VMEM((channels, depth), F32),
            pltpu.VMEM((seq_len, channels), F32),
            pltpu.VMEM((seq_len, channels), F32),
            pltpu.VMEM((seq_len, channels), F32),
            pltpu.VMEM(tile, F32),
            pltpu.VMEM(tile, F32),
            pltpu.VMEM(tile, F32),
            pltpu.VMEM(tile, F32),
            pltpu.VMEM((ROW, PART, BLK), BF16),
            pltpu.VMEM((n_dp, PART, BLK), BF16),
            pltpu.VMEM((n_dp, piece, channels), BF16),
            pltpu.VMEM((n_dp, piece, channels), BF16),
            pltpu.VMEM((PART, BLK), BF16),
            pltpu.VMEM((n_sp, PART, BLK), BF16),
            pltpu.VMEM((GROUPS * PART, BLK), BF16),
            pltpu.VMEM((ROW, GROUPS * PART, BLK), BF16),
            pltpu.VMEM((4, BLK), F32),
            pltpu.VMEM((n_dp, 4, BLK), F32),
            pltpu.VMEM((1, BLK), F32),
            pltpu.VMEM((n_sp, 1, BLK), F32),
            pltpu.VMEM((seq_len, channels), BF16),
            pltpu.VMEM((seq_len, channels), BF16),
            pltpu.VMEM(tile, BF16),
            pltpu.VMEM((GROUPS, BLK), BF16),
            pltpu.VMEM((1, channels), BF16),
            pltpu.VMEM((1, channels), BF16),
            dma((8,)),
            dma((chunks,)), dma((chunks,)), dma((chunks,)), dma((chunks,)),
            dma((n_dp,)), dma((n_dp,)),
            dma((n_sp,)), dma((n_sp,)), dma((n_sp,)), dma((n_sp,)),
            dma((n_sp,)), dma((n_sp,)), dma((n_sp,)), dma((n_sp,)),
            dma((n_dp,)), dma((n_dp,)), dma((n_dp,)), dma((n_dp,)),
            dma((n_sp,)), dma((n_sp,)), dma((ROW,)), dma((ROW,)),
            dma((n_dp,)), dma((n_dp,)), dma((n_sp,)), dma((n_sp,)),
            pltpu.SemaphoreType.REGULAR((3,)),
        ],
        compiler_params=pltpu.CompilerParams(
            collective_id=1, has_side_effects=True, vmem_limit_bytes=GRANT
        ),
    )(
        cotangent.reshape(2, BLK // 2, depth),
        unit_pre[0],
        gate_pre[0],
        out_weight,
        mix_weight,
        mix_bias,
        norm_gain[None],
        norm_shift[None],
    )
    outs = pl.pallas_call(
        put_out,
        out_shape=out_shapes,
        in_specs=[vmem] * 7,
        out_specs=(hbm,) * 7,
        scratch_shapes=[dma((7,))],
        compiler_params=pltpu.CompilerParams(vmem_limit_bytes=GRANT),
    )(*outs)
    unit_grad, gate_grad, out_grad, weight_total, bias_total, gain_total, shift_total = outs
    return (
        unit_grad[None],
        gate_grad[None],
        out_grad,
        weight_total,
        bias_total,
        gain_total[0],
        shift_total[0],
    )


def solution(mesh):
    return jax.shard_map(
        local,
        mesh=mesh,
        in_specs=(
            P("dp", "sp", None),
            P("dp", None, "sp"),
            P("dp", None, "sp"),
            P("dp", "sp"),
            P(),
            P(),
            P("sp"),
            P("sp"),
        ),
        out_specs=(P("dp", None, "sp"), P("dp", None, "sp"), P("dp", "sp"), P(), P(), P("sp"), P("sp")),
        check_vma=False,
    )
```
